128 devices in a mesh: sp: 16 (over z, y), dp: 8 (over x, core).
Axes of the slice: x: 4, y: 4, z: 4, core: 2. Of those that a mesh axis runs over, the one named last changes fastest.
Arguments:
- residual: bfloat16 [8, 2048, 2048], P('dp', 'sp'), may hold values from -6 to 6
- query_maps: bfloat16 [8, 2048, 2048], P('dp', 'sp'), may hold values from -200 to 200
- key_maps: bfloat16 [8, 2048, 2048], P('dp', 'sp'), may hold values from -200 to 200
- value_rows: bfloat16 [8, 2048, 2048], P('dp', 'sp'), may hold values from -6 to 6
- lambdas: float32 [16], replicated, may hold values from 0.3 to 0.8
- head_gain: float32 [2048], replicated, may hold values from 0.1 to 1.9
- out_weight: bfloat16 [2048, 2048], replicated, may hold values from -0.125 to 0.125
- ffn_gain: float32 [2048], replicated, may hold values from 0.1 to 1.9
- routes: int32 [8, 2048, 2], P('dp', 'sp'), may hold values from 0 to 127, all different within a row; in each aligned block of 128 rows (0 to 127, 128 to 255, ..., all dimensions but the last counted through in order) at most 4 rows name the same one
- route_weights: float32 [8, 2048, 2], P('dp', 'sp'), may hold values from 0.2 to 1
- expert_gate: bfloat16 [128, 2048, 1024], P(('sp', 'dp')), may hold values from -0.125 to 0.125
- expert_up: bfloat16 [128, 2048, 1024], P(('sp', 'dp')), may hold values from -0.125 to 0.125
- expert_down: bfloat16 [128, 1024, 2048], P(('sp', 'dp')), may hold values from -0.1875 to 0.1875
Outputs:
- layer_out: bfloat16 [8, 2048, 2048], P('dp', 'sp')
The draws below stay inside these ranges and needn't reach their ends.
Inputs may be any that keep to these rules, and one draw needn't show every extreme that they name: `routes`: A token's 2 experts differ; among the 128 rows of one device no expert is named more than 4 times, and in every draw some expert is named exactly 4 times by one device's rows.
All inputs are finite; a program needn't handle non-finite values.
Results may differ from the reference program's by a relative error of at most 0.012.
Values may be sent and summed in bfloat16 or wider, within the bound.
A program may use at most 128 MiB of HBM per device.

```python
import math
import jax
import jax.numpy as jnp
import numpy as np
from jax import lax

D = 2048
HEADS = 16
HD = 64
VD = 128
FF = 1024
TOPK = 2
TOK_DEV = 128
SEQ = 2048
EXPERTS = 128
CAP = 4
N_DP = 8


def base_keys(key):
    return 1.3 * jax.random.normal(jax.random.fold_in(key, 11), (N_DP, SEQ, HEADS * 2 * HD), jnp.float32)


def draw_key_maps(key, part):
    drawn = base_keys(key)
    return drawn.astype(jnp.bfloat16)


def draw_query_maps(key, part):
    drawn = 1.3 * jax.random.normal(jax.random.fold_in(key, 21), (N_DP, SEQ, HEADS * 2 * HD), jnp.float32)
    return drawn.astype(jnp.bfloat16)


def shard_levels(key, extent, split, least, largest):
    gain = 1.0
    for axis_at, shards_of in split:
        steps = jax.random.uniform(jax.random.fold_in(jax.random.fold_in(key, 6), axis_at), (shards_of,), jnp.float32, least / len(split), largest / len(split))
        gain = gain * jnp.repeat(jnp.exp(steps), extent[axis_at] // shards_of).reshape((-1,) + (1,) * (len(extent) - 1 - axis_at))
    return gain


def shared_out(own_key, own, number, rows, number_of, top, limit, skew):
    sequence = jax.random.permutation(own_key, number_of)
    crowded, usual = load_shares(number_of, rows * top, limit, skew, True), load_shares(number_of, rows * top, limit, skew, False)
    places = jnp.arange(number_of)

    def named(lengths, turn):
        used = int((lengths > 0).sum())
        fixed = max(1, used // 4)
        passed = fixed + (places - fixed + turn * (used - fixed)) % max(1, number_of - fixed)
        return jnp.zeros((number_of,), jnp.int32).at[sequence[jnp.where(places < fixed, places, passed)]].set(jnp.asarray(lengths, jnp.int32))

    lengths = jnp.where(number % 4 == 0, named(crowded, number // 4), named(usual, number - number // 4 - 1))
    mixed = jax.random.permutation(jax.random.fold_in(own, 3), number_of)
    giver, taker = mixed[0:number_of // 2 * 2:2], mixed[1:number_of // 2 * 2:2]
    slack = jnp.minimum(lengths[giver] - 1, limit - lengths[taker]) // 2
    slack = jnp.where((giver == sequence[0]) | (taker == sequence[0]) | (lengths[taker] == 0), 0, jnp.maximum(slack, 0))
    passed = jax.random.randint(jax.random.fold_in(own, 4), (number_of // 2,), 0, 1 << 20) % (slack + 1)
    lengths = lengths.at[giver].add(-passed).at[taker].add(passed)
    members = jnp.searchsorted(jnp.cumsum(lengths), jnp.arange(rows * top), side="right").astype(jnp.int32)
    table = members.reshape(top, rows).T
    table = table[jax.random.permutation(jax.random.fold_in(own, 1), rows)]
    turn = jax.random.randint(jax.random.fold_in(own, 2), (rows, 1), 0, top)
    return jnp.take_along_axis(table, (jnp.arange(top)[None, :] + turn) % top, axis=1)


def load_shares(count, total, bound, slope, full):
    weights = [(1 << 20) // math.isqrt(rank ** slope) + 1 for rank in range(1, count + 1)]
    largest = bound if full else min(bound, max(-(-total // count), total * weights[0] // sum(weights)))
    least = 1 if total - largest >= count - 1 else 0
    holding, spare = [largest] + [least] * (count - 1), total - largest - least * (count - 1)
    while spare > 0:
        candidates = [i for i in range(1, count) if holding[i] < largest] or [i for i in range(1, count) if holding[i] < bound]
        whole, remaining = sum([weights[i] for i in candidates]), spare
        for i in candidates:
            extra = min(bound - holding[i], max(1, remaining * weights[i] // whole), spare)
            holding[i] = holding[i] + extra
            spare = spare - extra
    return np.array(holding)


def scatter_about(rng, extent, scale, bound, shards=(), kind=jnp.bfloat16):
    gain = shard_levels(rng, extent, shards, -0.22, 0.18) if shards else 1.0
    values = jax.random.normal(rng, extent, jnp.float32) * scale * gain
    return jnp.minimum(jnp.maximum(values, -bound), bound).astype(kind)


def setup_inputs(seed: int = 0) -> dict:
    arg_keys = jax.random.split(jax.random.key(seed), 14)
    residual = scatter_about(arg_keys[0], (N_DP, SEQ, D), 1.0, 6.0, ((0, 8), (1, 16)))
    query_maps = draw_query_maps(jax.random.fold_in(arg_keys[13], 71), 0)
    key_maps = draw_key_maps(jax.random.fold_in(arg_keys[13], 71), 0)
    value_rows = scatter_about(arg_keys[3], (N_DP, SEQ, HEADS * VD), 1.0, 6.0, ((0, 8), (1, 16)))
    lambdas = jnp.clip(jax.random.uniform(arg_keys[4], (HEADS,), jnp.float32, 0.3, 0.8), 0.3, 0.8)
    head_gain = jnp.clip(1.0 + 0.18 * jax.random.normal(arg_keys[5], (HEADS * VD,), jnp.float32), 0.1, 1.9)
    out_weight = scatter_about(arg_keys[6], (HEADS * VD, D), (HEADS * VD) ** -0.5, 0.125)
    ffn_gain = jnp.clip(1.0 + 0.18 * jax.random.normal(arg_keys[7], (D,), jnp.float32), 0.1, 1.9)
    routes_keys = jax.random.split(jax.random.fold_in(arg_keys[8], 1), N_DP * SEQ // TOK_DEV)
    routes_turns = jax.random.permutation(jax.random.fold_in(arg_keys[8], 3), N_DP * SEQ // TOK_DEV)
    routes = jax.vmap(lambda own, number: shared_out(jax.random.fold_in(arg_keys[8], 2), own, number, TOK_DEV, EXPERTS, TOPK, CAP, 2))(routes_keys, routes_turns).reshape((N_DP, SEQ, TOPK))
    route_weights = jnp.clip(jnp.exp(math.log(1.0) - 1.609438 * jax.random.uniform(arg_keys[9], (N_DP, SEQ, TOPK), jnp.float32) ** shard_levels(arg_keys[9], (N_DP, SEQ, TOPK), ((0, 8), (1, 16)), -0.2, 0.2)), 0.2, 1.0)
    expert_gate = scatter_about(arg_keys[10], (EXPERTS, D, FF), D ** -0.5, 0.125, ((0, 128),))
    expert_up = scatter_about(arg_keys[11], (EXPERTS, D, FF), D ** -0.5, 0.125, ((0, 128),))
    expert_down = scatter_about(arg_keys[12], (EXPERTS, FF, D), FF ** -0.5, 0.1875, ((0, 128),))
    return {"residual": residual, "query_maps": query_maps, "key_maps": key_maps, "value_rows": value_rows, "lambdas": lambdas, "head_gain": head_gain, "out_weight": out_weight, "ffn_gain": ffn_gain, "routes": routes, "route_weights": route_weights, "expert_gate": expert_gate, "expert_up": expert_up, "expert_down": expert_down}


eps = 1e-06

def attend_head(query_head, key_head, value_head, lam_head, gain_head):
    length = query_head.shape[0]
    block_rows = min(512, length)
    count_blocks = length // block_rows
    scaling = query_head.shape[-1] ** (-0.5)
    query_blocks = query_head.reshape(count_blocks, block_rows, 2, query_head.shape[-1])
    keys_wide = key_head.astype(jnp.float32)

    def one_block(query_block):
        scores = jnp.einsum('qmd,kmd->mqk', query_block.astype(jnp.float32), keys_wide) * scaling
        probabilities = jax.nn.softmax(scores, axis=-1)
        mixed_map = (probabilities[0] - lam_head * probabilities[1]).astype(jnp.bfloat16)
        head_out = jnp.dot(mixed_map, value_head, preferred_element_type=jnp.float32)
        normed = head_out * lax.rsqrt(lax.optimization_barrier(jnp.mean(head_out * head_out, axis=-1, keepdims=True)) + eps)
        return (normed * gain_head * 0.8).astype(jnp.bfloat16)
    return lax.map(one_block, query_blocks).reshape(length, value_head.shape[-1])

def reference(residual, query_maps, key_maps, value_rows, lambdas, head_gain, out_weight, ffn_gain, routes, route_weights, expert_gate, expert_up, expert_down):
    items = N_DP * HEADS
    query_items = query_maps.reshape(N_DP, SEQ, HEADS, 2, HD).transpose(0, 2, 1, 3, 4).reshape(items, SEQ, 2, HD)
    key_items = key_maps.reshape(N_DP, SEQ, HEADS, 2, HD).transpose(0, 2, 1, 3, 4).reshape(items, SEQ, 2, HD)
    value_items = value_rows.reshape(N_DP, SEQ, HEADS, VD).transpose(0, 2, 1, 3).reshape(items, SEQ, VD)
    lam_items = jnp.tile(lambdas, N_DP)
    gain_items = jnp.tile(head_gain.reshape(HEADS, VD), (N_DP, 1))

    def per_item(packed):
        return attend_head(packed[0], packed[1], packed[2], packed[3], packed[4])
    attended = lax.map(per_item, (query_items, key_items, value_items, lam_items, gain_items))
    attended = attended.reshape(N_DP, HEADS, SEQ, VD).transpose(0, 2, 1, 3).reshape(N_DP * SEQ, HEADS * VD)
    total_rows = N_DP * SEQ
    projected = jnp.dot(attended, out_weight, preferred_element_type=jnp.float32)
    residual_mid = (residual.reshape(total_rows, D).astype(jnp.float32) + projected).astype(jnp.bfloat16)
    middle = residual_mid.astype(jnp.float32)
    expert_input = (middle * lax.rsqrt(lax.optimization_barrier(jnp.mean(middle * middle, axis=-1, keepdims=True)) + eps) * ffn_gain).astype(jnp.bfloat16)
    count_blocks = total_rows // TOK_DEV
    block_routes = routes.reshape(count_blocks, TOK_DEV * TOPK)

    def rank_block(route_block):
        onehot = (route_block[:, None] == jnp.arange(EXPERTS, dtype=jnp.int32)[None, :]).astype(jnp.int32)
        before = jnp.cumsum(onehot, axis=0) - onehot
        return lax.optimization_barrier(jnp.sum(before * onehot, axis=1))
    rank_of = lax.map(rank_block, block_routes).reshape(-1)
    flat_routes = routes.reshape(-1).astype(jnp.int32)
    token_of = (jnp.arange(total_rows * TOPK, dtype=jnp.int32) // TOPK).astype(jnp.int32)
    column = token_of // TOK_DEV * CAP + rank_of
    slot_table = jnp.full((EXPERTS, count_blocks * CAP), total_rows, jnp.int32).at[flat_routes, column].set(token_of)
    weight_table = jnp.zeros((EXPERTS, count_blocks * CAP), jnp.float32).at[flat_routes, column].set(route_weights.reshape(-1))
    padded_input = jnp.concatenate([expert_input, jnp.zeros((1, D), jnp.bfloat16)], axis=0)

    def per_expert(accumulated, packed):
        table_row, weight_row, gate_weight, up_weight, down_weight = packed
        row_block = padded_input[table_row]
        gate_part = jnp.dot(row_block, gate_weight, preferred_element_type=jnp.float32)
        up_part = jnp.dot(row_block, up_weight, preferred_element_type=jnp.float32)
        hidden = (jax.nn.silu(gate_part) * up_part).astype(jnp.bfloat16)
        expert_out = jnp.dot(hidden, down_weight, preferred_element_type=jnp.float32).astype(jnp.bfloat16)
        accumulated = accumulated.at[table_row].add(weight_row[:, None] * expert_out.astype(jnp.float32))
        return (accumulated, None)
    start_sum = jnp.zeros((total_rows + 1, D), jnp.float32)
    accumulated, _ = lax.scan(per_expert, start_sum, (slot_table, weight_table, expert_gate, expert_up, expert_down))
    layer_out = (middle + accumulated[:total_rows]).astype(jnp.bfloat16)
    return layer_out.reshape(N_DP, SEQ, D)
```

```python
import jax
import jax.numpy as jnp
from jax import lax
from jax.experimental import pallas as pl
from jax.experimental.pallas import tpu as pltpu
from jax.sharding import PartitionSpec as P

D = 2048
HEADS = 16
HD = 64
VD = 128
TOK = 128
SEQ = 2048
QB = 256
STEPS = SEQ // QB
KC = 256
RB = 16
MESH = pl.DeviceIdType.MESH
SP_DP = ("sp", "dp")
eps = 1e-06
LOG2E = 1.4426950408889634
NEAR = {0: 0, 1: 1, 2: 2, 3: 1}
PEERS = sorted(
    [(a, b) for a in range(4) for b in range(4) if (a, b) != (0, 0)],
    key=lambda o: -(NEAR[o[0]] + NEAR[o[1]]),
)


def peer_of(me, off):
    return ((me // 4 + off[0]) % 4) * 4 + (me % 4 + off[1]) % 4


def source_of(me, off):
    return ((me // 4 + 4 - off[0]) % 4) * 4 + (me % 4 + 4 - off[1]) % 4


def cols(block):
    return pl.ds(pl.multiple_of(block * VD, VD), VD)


def attention_kernel(
    q_ref, k_ref, v_ref, lam_ref, gain_ref, att_ref,
    qa, ka, va, s1a, s2a, s1b, s2b, pbuf, obuf,
    qs, ks, vs, qr, kr, vr, os_, or_, lsem,
):
    me = lax.axis_index("sp")
    barrier = pltpu.get_barrier_semaphore()
    for off in PEERS:
        pl.semaphore_signal(barrier, inc=1, device_id={"sp": peer_of(me, off)}, device_id_type=MESH)
    pl.semaphore_wait(barrier, len(PEERS))
    mine = cols(me)
    sends = []
    for n, (src, dst, ss, rs) in enumerate(((k_ref, ka, ks, kr), (v_ref, va, vs, vr), (q_ref, qa, qs, qr))):
        for i, off in enumerate(PEERS):
            to = peer_of(me, off)
            copy = pltpu.make_async_remote_copy(
                src.at[:, cols(to)], dst.at[mine, :], ss.at[i], rs.at[i],
                device_id={"sp": to}, device_id_type=MESH,
            )
            copy.start()
            sends.append(copy)
        own = pltpu.make_async_copy(src.at[:, mine], dst.at[mine, :], lsem.at[n])
        own.start()
        own.wait()
    count = len(PEERS)
    for copy in sends[: 2 * count]:
        copy.wait_recv()
    for copy in sends[2 * count :]:
        copy.wait_recv()
    lam = lam_ref[me]
    gain = gain_ref[pl.ds(me, 1), :] * 0.8
    first = lax.broadcasted_iota(jnp.int32, (QB, VD), 1) < HD
    scale = HD ** (-0.5) * LOG2E

    def scores(step, s1, s2):
        q = qa[pl.ds(pl.multiple_of(step * QB, QB), QB), :]
        zero = jnp.zeros_like(q)
        q1 = jnp.where(first, q, zero)
        q2 = jnp.where(first, zero, q)
        for c in range(SEQ // KC):
            k = ka[c * KC : (c + 1) * KC, :]
            at = pl.ds(c * KC, KC)
            dims = (((1,), (1,)), ((), ()))
            s1[:, at] = lax.dot_general(q1, k, dims, preferred_element_type=jnp.float32)
            s2[:, at] = lax.dot_general(q2, k, dims, preferred_element_type=jnp.float32)

    def mixed(step, s1, s2):
        inv = []
        for r in range(QB // RB):
            at = pl.ds(r * RB, RB)
            a = s1[at, :]
            e1 = jnp.exp2((a - jnp.max(a, axis=1, keepdims=True)) * scale)
            l1 = jnp.sum(e1, axis=1, keepdims=True)
            b = s2[at, :]
            e2 = jnp.exp2((b - jnp.max(b, axis=1, keepdims=True)) * scale)
            l2 = jnp.sum(e2, axis=1, keepdims=True)
            pbuf[at, :] = (e1 - e2 * (lam * l1 / l2)).astype(jnp.bfloat16)
            inv.append(1.0 / l1)
        out = jnp.dot(pbuf[...], va[...], preferred_element_type=jnp.float32)
        out = out * jnp.concatenate(inv, axis=0)
        out = out * lax.rsqrt(jnp.mean(out * out, axis=1, keepdims=True) + eps) * gain
        obuf[pl.ds(pl.multiple_of(step * QB, QB), QB), :] = out.astype(jnp.bfloat16)

    def pair(i, carry):
        step = 2 * i
        scores(step + 1, s1b, s2b)
        mixed(step, s1a, s2a)
        scores((step + 2) % STEPS, s1a, s2a)
        mixed(step + 1, s1b, s2b)
        return carry

    scores(0, s1a, s2a)
    lax.fori_loop(0, STEPS // 2, pair, 0)
    outs = []
    for i, off in enumerate(PEERS):
        to = peer_of(me, off)
        copy = pltpu.make_async_remote_copy(
            obuf.at[cols(to), :], att_ref.at[:, mine], os_.at[i], or_.at[i],
            device_id={"sp": to}, device_id_type=MESH,
        )
        copy.start()
        outs.append(copy)
    own = pltpu.make_async_copy(obuf.at[mine, :], att_ref.at[:, mine], lsem.at[3])
    own.start()
    own.wait()
    for copy in outs:
        copy.wait_recv()
    for copy in sends + outs:
        copy.wait_send()


def attention(q, k, v, lambdas, gain):
    n = len(PEERS)
    vmem = pl.BlockSpec(memory_space=pltpu.VMEM)
    smem = pl.BlockSpec(memory_space=pltpu.SMEM)
    score = pltpu.VMEM((QB, SEQ), jnp.float32)
    rows = pltpu.VMEM((SEQ, VD), jnp.bfloat16)
    return pl.pallas_call(
        attention_kernel,
        out_shape=jax.ShapeDtypeStruct((TOK, D), jnp.bfloat16),
        in_specs=[vmem, vmem, vmem, smem, vmem],
        out_specs=vmem,
        scratch_shapes=[rows, rows, rows, score, score, score, score,
                        pltpu.VMEM((QB, SEQ), jnp.bfloat16), rows]
        + [pltpu.SemaphoreType.DMA((n,))] * 8 + [pltpu.SemaphoreType.DMA((4,))],
        compiler_params=pltpu.CompilerParams(
            collective_id=0, has_side_effects=True, vmem_limit_bytes=56 * 2**20
        ),
        name="attention",
    )(q, k, v, lambdas, gain)


def in_blocks(value, dim, size):
    lengths = value.shape
    blocks = value.reshape(*lengths[:dim], size, lengths[dim] // size, *lengths[dim + 1 :])
    return jnp.moveaxis(blocks, dim, 0)


def laid_out(blocks, dim):
    blocks = jnp.moveaxis(blocks, 0, dim)
    lengths = blocks.shape
    return blocks.reshape(*lengths[:dim], lengths[dim] * lengths[dim + 1], *lengths[dim + 2 :])


def exchange_both(value, axis, axes, splits, concats):
    sizes = [lax.axis_size(a) for a in axes]
    blocks = in_blocks(value, splits[0], sizes[0])
    blocks = jnp.moveaxis(in_blocks(blocks, splits[1] + 1, sizes[1]), 0, 1)
    inside = blocks.shape[2:]
    blocks = blocks.reshape(-1, *inside)
    blocks = lax.all_to_all(blocks, axis, split_axis=0, concat_axis=0, tiled=True)
    blocks = laid_out(blocks.reshape(*sizes, *inside), concats[0] + 1)
    return laid_out(blocks, concats[1])


def on_device(
    residual, query_maps, key_maps, value_rows, lambdas, head_gain, out_weight, ffn_gain,
    routes, route_weights, expert_gate, expert_up, expert_down,
):
    count_sp = lax.axis_size("sp")
    count_dp = lax.axis_size("dp")
    returned_heads = attention(
        query_maps[0], key_maps[0], value_rows[0], lambdas, head_gain.reshape(HEADS, VD)
    )
    projected = jnp.dot(returned_heads, out_weight, preferred_element_type=jnp.float32)
    residual_mid = (residual[0].astype(jnp.float32) + projected).astype(jnp.bfloat16)
    middle = residual_mid.astype(jnp.float32)
    expert_input = (
        middle * lax.rsqrt(jnp.mean(middle * middle, axis=-1, keepdims=True) + eps) * ffn_gain
    ).astype(jnp.bfloat16)
    tok_rows = residual.shape[1]
    experts_all = count_sp * count_dp
    capacity = max(2, 4 * tok_rows // experts_all)
    flat_routes = routes[0].reshape(-1)
    flat_weights = route_weights[0].reshape(-1)
    onehot = (flat_routes[:, None] == jnp.arange(experts_all, dtype=jnp.int32)[None, :]).astype(
        jnp.int32
    )
    before = jnp.cumsum(onehot, axis=0) - onehot
    rank_of = jnp.sum(before * onehot, axis=1)
    slot = flat_routes * capacity + rank_of
    token_of = jnp.arange(flat_routes.shape[0], dtype=jnp.int32) // routes.shape[2]
    slot_token = jnp.full((experts_all * capacity,), tok_rows, jnp.int32).at[slot].set(token_of)
    padded_input = jnp.concatenate([expert_input, jnp.zeros((1, D), jnp.bfloat16)], axis=0)
    buffer = padded_input[slot_token].reshape(experts_all, capacity, D)
    shaped = buffer.reshape(count_sp, count_dp, capacity, D)
    received = exchange_both(shaped, SP_DP, ("sp", "dp"), (0, 1), (0, 1))
    row_block = received.reshape(-1, D)
    gate_part = jnp.dot(row_block, expert_gate[0], preferred_element_type=jnp.float32)
    up_part = jnp.dot(row_block, expert_up[0], preferred_element_type=jnp.float32)
    hidden = (jax.nn.silu(gate_part) * up_part).astype(jnp.bfloat16)
    expert_out = jnp.dot(hidden, expert_down[0], preferred_element_type=jnp.float32).astype(
        jnp.bfloat16
    )
    returned = exchange_both(expert_out.reshape(received.shape), SP_DP, ("sp", "dp"), (0, 1), (0, 1))
    picked = returned.reshape(experts_all * capacity, D)[slot]
    weighted = (picked.astype(jnp.float32) * flat_weights[:, None]).reshape(
        tok_rows, routes.shape[2], D
    )
    layer_out = (middle + jnp.sum(weighted, axis=1)).astype(jnp.bfloat16)
    return layer_out[None]


def solution(mesh):
    tokens = P("dp", "sp", None)
    experts = P(SP_DP, None, None)
    placed = (tokens,) * 4 + (P(),) * 4 + (tokens,) * 2 + (experts,) * 3
    return jax.shard_map(
        on_device, mesh=mesh, in_specs=placed, out_specs=tokens, check_vma=False
    )
```

```python
import jax
import jax.numpy as jnp
from jax import lax
from jax.experimental import pallas as pl
from jax.experimental.pallas import tpu as pltpu
from jax.sharding import PartitionSpec as P

D = 2048
HEADS = 16
HD = 64
VD = 128
FF = 1024
TOK = 128
SEQ = 2048
EXPERTS = 128
CAP = 4
SLOTS = EXPERTS * CAP
QB = 256
STEPS = SEQ // QB
KC = 256
RB = 16
NC = 512
GROUP = 32
MESH = pl.DeviceIdType.MESH
eps = 1e-06
LOG2E = 1.4426950408889634
F32 = jnp.float32
BF16 = jnp.bfloat16
NEAR = {0: 0, 1: 1, 2: 2, 3: 1}
PEERS = sorted(
    [(a, b) for a in range(4) for b in range(4) if (a, b) != (0, 0)],
    key=lambda o: -(NEAR[o[0]] + NEAR[o[1]]),
)
INNER = [(a, b, c) for a in (2, 3, 0, 1) for b in (2, 3, 0, 1) for c in (0, 1)]
OWN_GROUP, OWN_AT = 2, INNER.index((0, 0, 0))


def peer_of(me, off):
    return ((me // 4 + off[0]) % 4) * 4 + (me % 4 + off[1]) % 4


def minus(off):
    return tuple((4 - o) % 4 for o in off)


def chip_core(me, dx, dc):
    return ((me // 2 + dx) % 4) * 2 + (me % 2 + dc) % 2


def cols(block):
    return pl.ds(pl.multiple_of(block * VD, VD), VD)


def rows_of(step, size):
    return pl.ds(pl.multiple_of(step * size, size), size)


def layer_kernel(
    q_ref, k_ref, v_ref, res_ref, lam_ref, gain_ref, ffn_ref, route_ref, weight_ref,
    wo_hbm, wg_hbm, wu_hbm, wd_hbm,
    out_ref,
    qa, ka, va, s1a, s2a, s1b, s2b, pbuf, obuf, att, mid, xin, onehot, chigh, clow,
    wo, wg, wu, wd, xs, rx, hid, yx, ret,
    ks, kr, vs, vr, qs, qr, os_, or_, ds, dr, es, er, lsem, wsem,
):
    sp = lax.axis_index("sp")
    dp = lax.axis_index("dp")
    expert = sp * 8 + dp
    barrier = pltpu.get_barrier_semaphore()

    def device(dx, off):
        return {"sp": peer_of(sp, off[:2]), "dp": chip_core(dp, dx, off[2])}

    for g in range(4):
        for j, off in enumerate(INNER):
            if (g, j) != (OWN_GROUP, OWN_AT):
                pl.semaphore_signal(
                    barrier, inc=1, device_id=device((2 - g) % 4, off), device_id_type=MESH
                )
    pl.semaphore_wait(barrier, 127)

    mine = cols(sp)
    sends = []
    for src, dst, ss, rs in ((k_ref, ka, ks, kr), (v_ref, va, vs, vr)):
        for i, off in enumerate(PEERS):
            to = peer_of(sp, off)
            copy = pltpu.make_async_remote_copy(
                src.at[:, cols(to)], dst.at[mine, :], ss.at[i], rs.at[i],
                device_id={"sp": to}, device_id_type=MESH,
            )
            copy.start()
            sends.append(copy)
        own = pltpu.make_async_copy(src.at[:, mine], dst.at[mine, :], rs.at[15])
        own.start()
        sends.append(own)

    def query_copy(i, b):
        to = 2 * ((sp // 2 + 8 - i) % 8) + b
        at = 2 * i + b
        return to, pltpu.make_async_remote_copy(
            q_ref.at[:, cols(to)], qa.at[mine, :], qs.at[at], qr.at[2 * i + sp % 2],
            device_id={"sp": to}, device_id_type=MESH,
        )

    for i in range(STEPS):
        for b in range(2):
            to, copy = query_copy(i, b)
            if i == 0:
                pl.when(to != sp)(copy.start)
            else:
                copy.start()
    own_query = pltpu.make_async_copy(q_ref.at[:, mine], qa.at[mine, :], qr.at[sp % 2])
    own_query.start()
    loads = []
    for i, (src, dst) in enumerate(((wo_hbm, wo), (wg_hbm, wg), (wu_hbm, wu), (wd_hbm, wd))):
        load = pltpu.make_async_copy(src, dst, wsem.at[i])
        load.start()
        loads.append(load)

    lanes = lax.broadcasted_iota(jnp.int32, (TOK, EXPERTS), 1)
    lower = (lax.broadcasted_iota(jnp.int32, (TOK, TOK), 0) > lax.broadcasted_iota(jnp.int32, (TOK, TOK), 1))
    lower = jnp.where(lower, 1.0, 0.0).astype(BF16)
    slot_lanes = lax.broadcasted_iota(jnp.int32, (TOK, SLOTS), 1).astype(F32)
    ahead = jnp.zeros((1, EXPERTS), F32)
    rows_mark = jnp.zeros((TOK, SLOTS), F32)
    combine = jnp.zeros((TOK, SLOTS), F32)
    for k in range(2):
        named = route_ref[:, k : k + 1]
        mark = jnp.where(named == lanes, 1.0, 0.0)
        before = jnp.dot(lower, mark.astype(BF16), preferred_element_type=F32) + ahead
        rank = jnp.sum(before * mark, axis=1, keepdims=True)
        slot = named.astype(F32) * CAP + rank
        here = slot == slot_lanes
        rows_mark = jnp.where(here, 1.0, rows_mark)
        combine = jnp.where(here, weight_ref[:, k : k + 1], combine)
        ahead = ahead + jnp.sum(mark, axis=0, keepdims=True)
    onehot[...] = rows_mark.astype(BF16)
    high = combine.astype(BF16)
    chigh[...] = high
    clow[...] = (combine - high.astype(F32)).astype(BF16)

    for copy in sends:
        if hasattr(copy, "wait_recv") and copy.is_remote:
            copy.wait_recv()
        else:
            copy.wait()

    lam = lam_ref[sp]
    gain = gain_ref[pl.ds(sp, 1), :] * 0.8
    first = lax.broadcasted_iota(jnp.int32, (QB, VD), 1) < HD
    scale = HD ** (-0.5) * LOG2E

    def pair_of(step):
        return (sp // 2 + step) % STEPS

    def queries_arrive(step):
        for b in range(2):
            pltpu.make_async_remote_copy(
                q_ref.at[:, mine], qa.at[cols(2 * pair_of(step) + b), :],
                qs.at[2 * step + b], qr.at[2 * step + b],
                device_id={"sp": sp}, device_id_type=MESH,
            ).wait_recv()

    def scores(step, s1, s2):
        q = qa[rows_of(pair_of(step), QB), :]
        zero = jnp.zeros_like(q)
        q1 = jnp.where(first, q, zero)
        q2 = jnp.where(first, zero, q)
        dims = (((1,), (1,)), ((), ()))
        for c in range(SEQ // KC):
            k = ka[c * KC : (c + 1) * KC, :]
            at = pl.ds(c * KC, KC)
            s1[:, at] = lax.dot_general(q1, k, dims, preferred_element_type=F32)
            s2[:, at] = lax.dot_general(q2, k, dims, preferred_element_type=F32)

    def mixed(step, s1, s2):
        inv = []
        for r in range(QB // RB):
            at = pl.ds(r * RB, RB)
            a = s1[at, :]
            e1 = jnp.exp2((a - jnp.max(a, axis=1, keepdims=True)) * scale)
            l1 = jnp.sum(e1, axis=1, keepdims=True)
            b = s2[at, :]
            e2 = jnp.exp2((b - jnp.max(b, axis=1, keepdims=True)) * scale)
            l2 = jnp.sum(e2, axis=1, keepdims=True)
            pbuf[at, :] = (e1 - e2 * (lam * l1 / l2)).astype(BF16)
            inv.append(1.0 / l1)
        out = jnp.dot(pbuf[...], va[...], preferred_element_type=F32)
        out = out * jnp.concatenate(inv, axis=0)
        out = out * lax.rsqrt(jnp.mean(out * out, axis=1, keepdims=True) + eps) * gain
        obuf[rows_of(pair_of(step), QB), :] = out.astype(BF16)

    def head_copy(to):
        return pltpu.make_async_remote_copy(
            obuf.at[cols(to), :], att.at[:, mine], os_.at[to], or_.at[sp],
            device_id={"sp": to}, device_id_type=MESH,
        )

    own_head = pltpu.make_async_copy(obuf.at[mine, :], att.at[:, mine], or_.at[sp])

    def heads_leave(step):
        for b in range(2):
            to = 2 * pair_of(step) + b
            pl.when(to != sp)(head_copy(to).start)
            pl.when(to == sp)(own_head.start)

    def pair(i, carry):
        step = 2 * i
        queries_arrive(step + 1)
        scores(step + 1, s1b, s2b)
        mixed(step, s1a, s2a)
        heads_leave(step)

        @pl.when(i < STEPS // 2 - 1)
        def _():
            queries_arrive(step + 2)

        scores((step + 2) % STEPS, s1a, s2a)
        mixed(step + 1, s1b, s2b)
        heads_leave(step + 1)
        return carry

    queries_arrive(0)
    scores(0, s1a, s2a)
    lax.fori_loop(0, STEPS // 2, pair, 0)

    for h in range(HEADS):
        pltpu.make_async_remote_copy(
            obuf.at[mine, :], att.at[:, h * VD : (h + 1) * VD], os_.at[h], or_.at[h],
            device_id={"sp": sp}, device_id_type=MESH,
        ).wait_recv()

    loads[0].wait()
    squares = jnp.zeros((TOK, 1), F32)
    for n in range(D // NC):
        at = slice(n * NC, (n + 1) * NC)
        projected = jnp.dot(att[...], wo[:, at], preferred_element_type=F32)
        whole = (res_ref[:, at].astype(F32) + projected).astype(BF16)
        mid[:, at] = whole
        whole = whole.astype(F32)
        squares = squares + jnp.sum(whole * whole, axis=1, keepdims=True)
    inverse = lax.rsqrt(squares * (1.0 / D) + eps)
    for n in range(D // NC):
        at = slice(n * NC, (n + 1) * NC)
        x = (mid[:, at].astype(F32) * inverse * ffn_ref[:, at]).astype(BF16)
        picked = lax.dot_general(
            onehot[...], x, (((0,), (0,)), ((), ())), preferred_element_type=F32
        ).astype(BF16)
        xs[:, :, at] = picked.reshape(EXPERTS, CAP, NC)

    for g in range(4):
        dx = (2 - g) % 4
        for j, off in enumerate(INNER):
            i = g * GROUP + j
            if (g, j) == (OWN_GROUP, OWN_AT):
                pltpu.make_async_copy(xs.at[expert], rx.at[i], dr.at[i]).start()
                continue
            to = device(dx, off)
            pltpu.make_async_remote_copy(
                xs.at[to["sp"] * 8 + to["dp"]], rx.at[i], ds.at[i], dr.at[i],
                device_id=to, device_id_type=MESH,
            ).start()
    for load in loads[1:]:
        load.wait()

    def dispatch_wait(i):
        return pltpu.make_async_remote_copy(
            xs.at[0], rx.at[i], ds.at[i], dr.at[i],
            device_id={"sp": sp}, device_id_type=MESH,
        )

    def batch(g, carry):
        at = rows_of(g, GROUP)
        for j in range(GROUP):
            dispatch_wait(g * GROUP + j).wait_recv()
        x = rx[at].reshape(GROUP * CAP, D)
        for n in range(FF // 256):
            w = slice(n * 256, (n + 1) * 256)
            gate = jnp.dot(x, wg[:, w], preferred_element_type=F32)
            up = jnp.dot(x, wu[:, w], preferred_element_type=F32)
            hid[:, w] = (gate / (1.0 + jnp.exp(-gate)) * up).astype(BF16)
        h = hid[...]
        for n in range(D // NC):
            w = slice(n * NC, (n + 1) * NC)
            y = jnp.dot(h, wd[:, w], preferred_element_type=F32).astype(BF16)
            yx[at, :, w] = y.reshape(GROUP, CAP, NC)
        dx = (g + 2) % 4
        for j, off in enumerate(INNER):
            i = g * GROUP + j
            back = pltpu.make_async_remote_copy(
                yx.at[i], ret.at[expert], es.at[i], er.at[i],
                device_id={
                    "sp": peer_of(sp, minus(off[:2])),
                    "dp": chip_core(dp, dx, off[2]),
                },
                device_id_type=MESH,
            )
            if j == OWN_AT:
                own = pltpu.make_async_copy(yx.at[i], ret.at[expert], er.at[i])
                pl.when(g != OWN_GROUP)(back.start)
                pl.when(g == OWN_GROUP)(own.start)
            else:
                back.start()
        return carry

    lax.fori_loop(0, 4, batch, 0)

    def returned(i):
        return pltpu.make_async_remote_copy(
            yx.at[i], ret.at[0], es.at[i], er.at[i],
            device_id={"sp": sp}, device_id_type=MESH,
        )

    for i in range(EXPERTS):
        returned(i).wait_recv()
    for n in range(D // NC):
        at = slice(n * NC, (n + 1) * NC)
        r = ret[:, :, at].reshape(SLOTS, NC)
        total = jnp.dot(chigh[...], r, preferred_element_type=F32)
        total = total + jnp.dot(clow[...], r, preferred_element_type=F32)
        out_ref[:, at] = (mid[:, at].astype(F32) + total).astype(BF16)

    for copy in sends:
        if copy.is_remote:
            copy.wait_send()
    for i in range(STEPS):
        for b in range(2):
            to, copy = query_copy(i, b)
            if i == 0:
                pl.when(to != sp)(copy.wait_send)
            else:
                copy.wait_send()
    for h in range(HEADS):
        pl.when(sp != h)(head_copy(h).wait_send)
    for i in range(EXPERTS):
        if i != OWN_GROUP * GROUP + OWN_AT:
            dispatch_wait(i).wait_send()
            returned(i).wait_send()


def on_device(
    residual, query_maps, key_maps, value_rows, lambdas, head_gain, out_weight, ffn_gain,
    routes, route_weights, expert_gate, expert_up, expert_down,
):
    vmem = pl.BlockSpec(memory_space=pltpu.VMEM)
    smem = pl.BlockSpec(memory_space=pltpu.SMEM)
    hbm = pl.BlockSpec(memory_space=pl.ANY)
    score = pltpu.VMEM((QB, SEQ), F32)
    rows = pltpu.VMEM((SEQ, VD), BF16)
    tokens = pltpu.VMEM((TOK, D), BF16)
    table = pltpu.VMEM((TOK, SLOTS), BF16)
    slots = pltpu.VMEM((EXPERTS, CAP, D), BF16)
    sem = pltpu.SemaphoreType.DMA
    out = pl.pallas_call(
        layer_kernel,
        out_shape=jax.ShapeDtypeStruct((TOK, D), BF16),
        in_specs=[vmem] * 4 + [smem] + [vmem] * 4 + [hbm] * 4,
        out_specs=vmem,
        scratch_shapes=[rows, rows, rows, score, score, score, score,
                        pltpu.VMEM((QB, SEQ), BF16), rows, tokens, tokens, tokens,
                        table, table, table,
                        pltpu.VMEM((D, D), BF16), pltpu.VMEM((D, FF), BF16),
                        pltpu.VMEM((D, FF), BF16), pltpu.VMEM((FF, D), BF16),
                        slots, slots, pltpu.VMEM((GROUP * CAP, FF), BF16), slots, slots]
        + [sem((16,))] * 8 + [sem((EXPERTS,))] * 4 + [sem((4,))] * 2,
        compiler_params=pltpu.CompilerParams(
            collective_id=0, has_side_effects=True, vmem_limit_bytes=60 * 2**20
        ),
        name="layer",
    )(
        query_maps[0], key_maps[0], value_rows[0], residual[0], lambdas,
        head_gain.reshape(HEADS, VD), ffn_gain.reshape(1, D), routes[0], route_weights[0],
        out_weight, expert_gate[0], expert_up[0], expert_down[0],
    )
    return out[None]


def solution(mesh):
    tokens = P("dp", "sp", None)
    experts = P(("sp", "dp"), None, None)
    placed = (tokens,) * 4 + (P(),) * 4 + (tokens,) * 2 + (experts,) * 3
    return jax.shard_map(
        on_device, mesh=mesh, in_specs=placed, out_specs=tokens, check_vma=False
    )
```

```python
import jax
import jax.numpy as jnp
from jax import lax
from jax.experimental import pallas as pl
from jax.experimental.pallas import tpu as pltpu
from jax.sharding import PartitionSpec as P

D = 2048
HEADS = 16
HD = 64
VD = 128
FF = 1024
TOK = 128
SEQ = 2048
EXPERTS = 128
CAP = 4
SLOTS = EXPERTS * CAP
QB = 256
STEPS = SEQ // QB
KC = 256
RB = 16
NC = 512
GROUP = 32
MESH = pl.DeviceIdType.MESH
eps = 1e-06
LOG2E = 1.4426950408889634
F32 = jnp.float32
BF16 = jnp.bfloat16
NEAR = {0: 0, 1: 1, 2: 2, 3: 1}
PEERS = sorted(
    [(a, b) for a in range(4) for b in range(4) if (a, b) != (0, 0)],
    key=lambda o: -(NEAR[o[0]] + NEAR[o[1]]),
)
INNER = [(a, b, c) for a, b in PEERS + [(0, 0)] for c in (1, 0)]
OWN_GROUP, OWN_AT = 0, INNER.index((0, 0, 0))


def peer_of(me, off):
    return ((me // 4 + off[0]) % 4) * 4 + (me % 4 + off[1]) % 4


def minus(off):
    return tuple((4 - o) % 4 for o in off)


def chip_core(me, dx, dc):
    return ((me // 2 + dx) % 4) * 2 + (me % 2 + dc) % 2


def cols(block):
    return pl.ds(pl.multiple_of(block * VD, VD), VD)


def rows_of(step, size):
    return pl.ds(pl.multiple_of(step * size, size), size)


def layer_kernel(
    q_hbm, k_hbm, v_hbm, res_hbm, lam_ref, gain_ref, ffn_ref, route_ref, weight_ref,
    wo_hbm, wg_hbm, wu_hbm, wd_hbm,
    out_ref,
    q_ref, k_ref, v_ref, res_ref,
    qa, ka, va, s1a, s2a, s1b, s2b, pbuf, obuf, att, mid, onehot, chigh, clow,
    wo, wg, wu, wd, xs, rx, hid, yx, ret,
    kvs, kvr, qs, qr, os_, or_, ds, dr, es, er, insem, wsem, ready,
):
    sp = lax.axis_index("sp")
    dp = lax.axis_index("dp")
    expert = sp * 8 + dp
    barrier = pltpu.get_barrier_semaphore()
    for off in PEERS:
        pl.semaphore_signal(barrier, inc=1, device_id={"sp": peer_of(sp, off)}, device_id_type=MESH)
    for i in range(1, 8):
        to = chip_core(dp, i // 2, i % 2)
        pl.semaphore_signal(barrier, inc=1, device_id={"dp": to}, device_id_type=MESH)
    inputs = []
    for i, (src, dst) in enumerate(((k_hbm, k_ref), (v_hbm, v_ref), (q_hbm, q_ref), (res_hbm, res_ref))):
        load = pltpu.make_async_copy(src, dst, insem.at[i])
        load.start()
        inputs.append(load)
    pl.semaphore_wait(barrier, 22)
    for off in PEERS:
        pl.semaphore_signal(ready, inc=1, device_id={"sp": peer_of(sp, off)}, device_id_type=MESH)

    mine = cols(sp)
    for n, (src, dst) in enumerate(((k_ref, ka), (v_ref, va))):
        inputs[n].wait()
        for off in PEERS:
            to = peer_of(sp, off)
            pltpu.make_async_remote_copy(
                src.at[:, cols(to)], dst.at[mine, :], kvs.at[n], kvr.at[n],
                device_id={"sp": to}, device_id_type=MESH,
            ).start()
        pltpu.make_async_copy(src.at[:, mine], dst.at[mine, :], kvr.at[n]).start()

    def query_copy(i, b):
        to = 2 * ((sp // 2 + 8 - i) % 8) + b
        return to, pltpu.make_async_remote_copy(
            q_ref.at[:, cols(to)], qa.at[mine, :], qs.at[2 * i + b], qr.at[2 * i + sp % 2],
            device_id={"sp": to}, device_id_type=MESH,
        )

    inputs[2].wait()
    pltpu.make_async_copy(q_ref.at[:, mine], qa.at[mine, :], qr.at[sp % 2]).start()
    for i in range(STEPS):
        for b in range(2):
            to, copy = query_copy(i, b)
            if i == 0:
                pl.when(to != sp)(copy.start)
            else:
                copy.start()
    loads = []
    for i, (src, dst) in enumerate(((wo_hbm, wo), (wg_hbm, wg), (wu_hbm, wu), (wd_hbm, wd))):
        load = pltpu.make_async_copy(src, dst, wsem.at[i])
        load.start()
        loads.append(load)

    names = lax.broadcasted_iota(jnp.int32, (EXPERTS, TOK), 0)
    earlier = lax.broadcasted_iota(jnp.int32, (TOK, TOK), 0) < lax.broadcasted_iota(jnp.int32, (TOK, TOK), 1)
    earlier = jnp.where(earlier, 1.0, 0.0).astype(BF16)
    slots = lax.broadcasted_iota(jnp.int32, (SLOTS, TOK), 0).astype(F32)
    ahead = jnp.zeros((EXPERTS, 1), F32)
    marks = jnp.zeros((SLOTS, TOK), F32)
    combine = jnp.zeros((SLOTS, TOK), F32)
    for k in range(2):
        named = route_ref[k : k + 1, :]
        mark = jnp.where(named == names, 1.0, 0.0)
        before = jnp.dot(mark.astype(BF16), earlier, preferred_element_type=F32) + ahead
        rank = jnp.sum(before * mark, axis=0, keepdims=True)
        here = named.astype(F32) * CAP + rank == slots
        marks = jnp.where(here, 1.0, marks)
        combine = jnp.where(here, weight_ref[k : k + 1, :], combine)
        ahead = ahead + jnp.sum(mark, axis=1, keepdims=True)
    onehot[...] = marks.astype(BF16)
    high = combine.astype(BF16)
    chigh[...] = high
    clow[...] = (combine - high.astype(F32)).astype(BF16)

    def all_blocks(src, dst, ss, rs, count):
        size = src.shape[0] // 16 * count
        return pltpu.make_async_remote_copy(
            src.at[pl.ds(0, size)], dst.at[pl.ds(0, size)], ss, rs,
            device_id={"sp": sp}, device_id_type=MESH,
        )

    all_blocks(ka, ka, kvs.at[0], kvr.at[0], 16).wait_recv()
    all_blocks(va, va, kvs.at[1], kvr.at[1], 16).wait_recv()

    lam = lam_ref[sp]
    gain = gain_ref[pl.ds(sp, 1), :] * 0.8
    first = lax.broadcasted_iota(jnp.int32, (QB, VD), 1) < HD
    scale = HD ** (-0.5) * LOG2E

    def pair_of(step):
        return (sp // 2 + step) % STEPS

    def queries_arrive(step):
        for b in range(2):
            pltpu.make_async_remote_copy(
                q_ref.at[:, mine], qa.at[cols(2 * pair_of(step) + b), :],
                qs.at[2 * step + b], qr.at[2 * step + b],
                device_id={"sp": sp}, device_id_type=MESH,
            ).wait_recv()

    def scores(step, s1, s2):
        q = qa[rows_of(pair_of(step), QB), :]
        zero = jnp.zeros_like(q)
        q1 = jnp.where(first, q, zero)
        q2 = jnp.where(first, zero, q)
        dims = (((1,), (1,)), ((), ()))
        for c in range(SEQ // KC):
            k = ka[c * KC : (c + 1) * KC, :]
            at = pl.ds(c * KC, KC)
            s1[:, at] = lax.dot_general(q1, k, dims, preferred_element_type=F32)
            s2[:, at] = lax.dot_general(q2, k, dims, preferred_element_type=F32)

    def mixed(step, s1, s2):
        inv = []
        for r in range(QB // RB):
            at = pl.ds(r * RB, RB)
            a = s1[at, :]
            e1 = jnp.exp2((a - jnp.max(a, axis=1, keepdims=True)) * scale)
            l1 = jnp.sum(e1, axis=1, keepdims=True)
            b = s2[at, :]
            e2 = jnp.exp2((b - jnp.max(b, axis=1, keepdims=True)) * scale)
            l2 = jnp.sum(e2, axis=1, keepdims=True)
            pbuf[at, :] = (e1 - e2 * (lam * l1 / l2)).astype(BF16)
            inv.append(1.0 / l1)
        out = jnp.dot(pbuf[...], va[...], preferred_element_type=F32)
        out = out * jnp.concatenate(inv, axis=0)
        out = out * lax.rsqrt(jnp.mean(out * out, axis=1, keepdims=True) + eps) * gain
        obuf[rows_of(pair_of(step), QB), :] = out.astype(BF16)

    def head_copy(to):
        return pltpu.make_async_remote_copy(
            obuf.at[cols(to), :], att.at[:, mine], os_, or_,
            device_id={"sp": to}, device_id_type=MESH,
        )

    own_head = pltpu.make_async_copy(obuf.at[mine, :], att.at[:, mine], or_)

    def heads_leave(step):
        for b in range(2):
            to = 2 * pair_of(step) + b
            pl.when(to != sp)(head_copy(to).start)
            pl.when(to == sp)(own_head.start)

    def pair(i, carry):
        step = 2 * i
        queries_arrive(step + 1)
        scores(step + 1, s1b, s2b)
        mixed(step, s1a, s2a)
        heads_leave(step)

        @pl.when(i < STEPS // 2 - 1)
        def _():
            queries_arrive(step + 2)

        scores((step + 2) % STEPS, s1a, s2a)
        mixed(step + 1, s1b, s2b)
        heads_leave(step + 1)
        return carry

    queries_arrive(0)
    scores(0, s1a, s2a)
    lax.fori_loop(0, STEPS // 2, pair, 0)

    inputs[3].wait()
    loads[0].wait()
    all_blocks(obuf, obuf, os_, or_, 16).wait_recv()

    squares = jnp.zeros((TOK, 1), F32)
    for n in range(D // NC):
        at = slice(n * NC, (n + 1) * NC)
        projected = jnp.dot(att[...], wo[:, at], preferred_element_type=F32)
        whole = (res_ref[:, at].astype(F32) + projected).astype(BF16)
        mid[:, at] = whole
        whole = whole.astype(F32)
        squares = squares + jnp.sum(whole * whole, axis=1, keepdims=True)
    inverse = lax.rsqrt(squares * (1.0 / D) + eps)
    for n in range(D // NC):
        at = slice(n * NC, (n + 1) * NC)
        x = (mid[:, at].astype(F32) * inverse * ffn_ref[:, at]).astype(BF16)
        picked = jnp.dot(onehot[...], x, preferred_element_type=F32).astype(BF16)
        xs[:, :, at] = picked.reshape(EXPERTS, CAP, NC)

    pl.semaphore_wait(ready, 15)
    peers = [peer_of(sp, off) for off in PEERS] + [sp]
    others = [[chip_core(dp, dx, dc) for dc in range(2)] for dx in range(4)]
    for g in range(4):
        for j, (dz, dy, dc) in enumerate(INNER):
            i = g * GROUP + j
            if (g, j) == (OWN_GROUP, OWN_AT):
                pltpu.make_async_copy(xs.at[expert], rx.at[i], dr.at[g]).start()
                continue
            to_sp, to_dp = peers[j // 2], others[(g + dz + dy) % 4][dc]
            pltpu.make_async_remote_copy(
                xs.at[to_sp * 8 + to_dp], rx.at[i], ds.at[g], dr.at[g],
                device_id={"sp": to_sp, "dp": to_dp}, device_id_type=MESH,
            ).start()
    for load in loads[1:]:
        load.wait()

    def whole_batch(src, dst, ss, rs, count):
        return pltpu.make_async_remote_copy(
            src.at[pl.ds(0, count)], dst.at[pl.ds(0, count)], ss, rs,
            device_id={"sp": sp}, device_id_type=MESH,
        )

    homes = [peer_of(sp, minus(off)) for off in PEERS] + [sp]

    def batch(g, carry):
        at = rows_of(g, GROUP)
        whole_batch(xs, rx, ds.at[g], dr.at[g], GROUP).wait_recv()
        x = rx[at].reshape(GROUP * CAP, D)
        for n in range(FF // 256):
            w = slice(n * 256, (n + 1) * 256)
            gate = jnp.dot(x, wg[:, w], preferred_element_type=F32)
            up = jnp.dot(x, wu[:, w], preferred_element_type=F32)
            hid[:, w] = (gate / (1.0 + jnp.exp(-gate)) * up).astype(BF16)
        h = hid[...]
        for n in range(D // NC):
            w = slice(n * NC, (n + 1) * NC)
            y = jnp.dot(h, wd[:, w], preferred_element_type=F32).astype(BF16)
            yx[at, :, w] = y.reshape(GROUP, CAP, NC)
        back_to = [[chip_core(dp, (8 - g - turn) % 4, dc) for dc in range(2)] for turn in range(4)]
        for j, (dz, dy, dc) in enumerate(INNER):
            i = g * GROUP + j
            back = pltpu.make_async_remote_copy(
                yx.at[i], ret.at[expert], es.at[g], er.at[g],
                device_id={"sp": homes[j // 2], "dp": back_to[(dz + dy) % 4][dc]},
                device_id_type=MESH,
            )
            if j == OWN_AT:
                own = pltpu.make_async_copy(yx.at[i], ret.at[expert], er.at[g])
                pl.when(g != OWN_GROUP)(back.start)
                pl.when(g == OWN_GROUP)(own.start)
            else:
                back.start()
        return carry

    lax.fori_loop(0, 4, batch, 0)

    for g in range(4):
        whole_batch(yx, ret, es.at[g], er.at[g], GROUP).wait_recv()
    for n in range(D // NC):
        at = slice(n * NC, (n + 1) * NC)
        r = ret[:, :, at].reshape(SLOTS, NC)
        dims = (((0,), (0,)), ((), ()))
        total = lax.dot_general(chigh[...], r, dims, preferred_element_type=F32)
        total = total + lax.dot_general(clow[...], r, dims, preferred_element_type=F32)
        out_ref[:, at] = (mid[:, at].astype(F32) + total).astype(BF16)

    all_blocks(ka, ka, kvs.at[0], kvr.at[0], 15).wait_send()
    all_blocks(va, va, kvs.at[1], kvr.at[1], 15).wait_send()
    all_blocks(obuf, obuf, os_, or_, 15).wait_send()
    for g in range(4):
        count = GROUP - (g == OWN_GROUP)
        whole_batch(xs, rx, ds.at[g], dr.at[g], count).wait_send()
        whole_batch(yx, ret, es.at[g], er.at[g], count).wait_send()
    for i in range(STEPS):
        for b in range(2):
            to, copy = query_copy(i, b)
            if i == 0:
                pl.when(to != sp)(copy.wait_send)
            else:
                copy.wait_send()


def on_device(
    residual, query_maps, key_maps, value_rows, lambdas, head_gain, out_weight, ffn_gain,
    routes, route_weights, expert_gate, expert_up, expert_down,
):
    vmem = pl.BlockSpec(memory_space=pltpu.VMEM)
    smem = pl.BlockSpec(memory_space=pltpu.SMEM)
    hbm = pl.BlockSpec(memory_space=pl.ANY)
    score = pltpu.VMEM((QB, SEQ), F32)
    rows = pltpu.VMEM((SEQ, VD), BF16)
    tokens = pltpu.VMEM((TOK, D), BF16)
    table = pltpu.VMEM((SLOTS, TOK), BF16)
    slots = pltpu.VMEM((EXPERTS, CAP, D), BF16)
    sem = pltpu.SemaphoreType.DMA
    out = pl.pallas_call(
        layer_kernel,
        out_shape=jax.ShapeDtypeStruct((TOK, D), BF16),
        in_specs=[hbm] * 4 + [smem] + [vmem] * 4 + [hbm] * 4,
        out_specs=vmem,
        scratch_shapes=[tokens] * 4 + [rows, rows, rows, score, score, score, score,
                        pltpu.VMEM((QB, SEQ), BF16), rows, tokens, tokens,
                        table, table, table,
                        pltpu.VMEM((D, D), BF16), pltpu.VMEM((D, FF), BF16),
                        pltpu.VMEM((D, FF), BF16), pltpu.VMEM((FF, D), BF16),
                        slots, slots, pltpu.VMEM((GROUP * CAP, FF), BF16), slots, slots]
        + [sem((2,)), sem((2,)), sem((16,)), sem((16,)), sem, sem] + [sem((4,))] * 6
        + [pltpu.SemaphoreType.REGULAR],
        compiler_params=pltpu.CompilerParams(
            collective_id=0, has_side_effects=True, vmem_limit_bytes=60 * 2**20
        ),
        name="layer",
    )(
        query_maps[0], key_maps[0], value_rows[0], residual[0], lambdas,
        head_gain.reshape(HEADS, VD), ffn_gain.reshape(1, D), routes[0].T, route_weights[0].T,
        out_weight, expert_gate[0], expert_up[0], expert_down[0],
    )
    return out[None]


def solution(mesh):
    tokens = P("dp", "sp", None)
    experts = P(("sp", "dp"), None, None)
    placed = (tokens,) * 4 + (P(),) * 4 + (tokens,) * 2 + (experts,) * 3
    return jax.shard_map(
        on_device, mesh=mesh, in_specs=placed, out_specs=tokens, check_vma=False
    )
```

```python
import jax
import jax.numpy as jnp
from jax import lax
from jax.experimental import pallas as pl
from jax.experimental.pallas import tpu as pltpu
from jax.sharding import PartitionSpec as P

D = 2048
HEADS = 16
HD = 64
VD = 128
FF = 1024
TOK = 128
SEQ = 2048
EXPERTS = 128
CAP = 4
SLOTS = EXPERTS * CAP
QB = 256
STEPS = SEQ // QB
HALF = STEPS // 2
KC = 256
RB = 16
NC = 512
GROUP = 32
MESH = pl.DeviceIdType.MESH
eps = 1e-06
LOG2E = 1.4426950408889634
F32 = jnp.float32
BF16 = jnp.bfloat16
NEAR = {0: 0, 1: 1, 2: 2, 3: 1}
PEERS = sorted(
    [(a, b) for a in range(4) for b in range(4) if (a, b) != (0, 0)],
    key=lambda o: -(NEAR[o[0]] + NEAR[o[1]]),
)
INNER = [(a, b, c) for a, b in PEERS + [(0, 0)] for c in (1, 0)]
OWN_GROUP, OWN_AT = 0, INNER.index((0, 0, 0))


def peer_of(me, off):
    return ((me // 4 + off[0]) % 4) * 4 + (me % 4 + off[1]) % 4


def minus(off):
    return tuple((4 - o) % 4 for o in off)


def chip_core(me, dx, dc):
    return ((me // 2 + dx) % 4) * 2 + (me % 2 + dc) % 2


def cols(block):
    return pl.ds(pl.multiple_of(block * VD, VD), VD)


def rows_of(step, size):
    return pl.ds(pl.multiple_of(step * size, size), size)


def layer_kernel(
    q_hbm, k_hbm, v_hbm, res_hbm, lam_ref, gain_ref, ffn_ref, route_ref, weight_ref,
    wo_hbm, wg_hbm, wu_hbm, wd_hbm,
    out_hbm,
    q_ref, k_ref, v_ref, res_ref,
    qa, ka, va, s1a, s2a, s1b, s2b, maps, sums, obuf, att, total, mid, out, onehot, chigh, clow,
    wo, wg, wu, wd, xs, rx, hid, yx, ret,
    kvs, kvr, qs, qr, os_, or_, ds, dr, es, er, insem, wsem, outsem, ready,
):
    sp = lax.axis_index("sp")
    dp = lax.axis_index("dp")
    expert = sp * 8 + dp
    barrier = pltpu.get_barrier_semaphore()
    for off in PEERS:
        pl.semaphore_signal(barrier, inc=1, device_id={"sp": peer_of(sp, off)}, device_id_type=MESH)
    for i in range(1, 8):
        to = chip_core(dp, i // 2, i % 2)
        pl.semaphore_signal(barrier, inc=1, device_id={"dp": to}, device_id_type=MESH)
    inputs = []
    for i, (src, dst) in enumerate(((k_hbm, k_ref), (v_hbm, v_ref), (q_hbm, q_ref), (res_hbm, res_ref))):
        load = pltpu.make_async_copy(src, dst, insem.at[i])
        load.start()
        inputs.append(load)
    pl.semaphore_wait(barrier, 22)
    for off in PEERS:
        pl.semaphore_signal(ready, inc=1, device_id={"sp": peer_of(sp, off)}, device_id_type=MESH)

    mine = cols(sp)

    def rows_leave(n, src, dst):
        inputs[n].wait()
        for off in PEERS:
            to = peer_of(sp, off)
            pltpu.make_async_remote_copy(
                src.at[:, cols(to)], dst.at[mine, :], kvs.at[n], kvr.at[n],
                device_id={"sp": to}, device_id_type=MESH,
            ).start()
        pltpu.make_async_copy(src.at[:, mine], dst.at[mine, :], kvr.at[n]).start()

    def query_copy(i, b):
        to = 2 * ((sp // 2 + 8 - i) % 8) + b
        return to, pltpu.make_async_remote_copy(
            q_ref.at[:, cols(to)], qa.at[mine, :], qs.at[2 * i + b], qr.at[2 * i + sp % 2],
            device_id={"sp": to}, device_id_type=MESH,
        )

    def queries_leave(steps):
        for i in steps:
            for b in range(2):
                to, copy = query_copy(i, b)
                if i == 0:
                    pl.when(to != sp)(copy.start)
                else:
                    copy.start()

    rows_leave(0, k_ref, ka)
    inputs[2].wait()
    pltpu.make_async_copy(q_ref.at[:, mine], qa.at[mine, :], qr.at[sp % 2]).start()
    queries_leave(range(HALF))
    rows_leave(1, v_ref, va)
    queries_leave(range(HALF, STEPS))
    loads = []
    for i, (src, dst) in enumerate(((wo_hbm, wo), (wg_hbm, wg), (wu_hbm, wu), (wd_hbm, wd))):
        load = pltpu.make_async_copy(src, dst, wsem.at[i])
        load.start()
        loads.append(load)

    names = lax.broadcasted_iota(jnp.int32, (EXPERTS, TOK), 0)
    earlier = lax.broadcasted_iota(jnp.int32, (TOK, TOK), 0) < lax.broadcasted_iota(jnp.int32, (TOK, TOK), 1)
    earlier = jnp.where(earlier, 1.0, 0.0).astype(BF16)
    slots = lax.broadcasted_iota(jnp.int32, (SLOTS, TOK), 0).astype(F32)
    ahead = jnp.zeros((EXPERTS, 1), F32)
    marks = jnp.zeros((SLOTS, TOK), F32)
    combine = jnp.zeros((SLOTS, TOK), F32)
    for k in range(2):
        named = route_ref[k : k + 1, :]
        mark = jnp.where(named == names, 1.0, 0.0)
        before = jnp.dot(mark.astype(BF16), earlier, preferred_element_type=F32) + ahead
        rank = jnp.sum(before * mark, axis=0, keepdims=True)
        here = named.astype(F32) * CAP + rank == slots
        marks = jnp.where(here, 1.0, marks)
        combine = jnp.where(here, weight_ref[k : k + 1, :], combine)
        ahead = ahead + jnp.sum(mark, axis=1, keepdims=True)
    onehot[...] = marks.astype(BF16)
    high = combine.astype(BF16)
    chigh[...] = high
    clow[...] = (combine - high.astype(F32)).astype(BF16)

    def all_blocks(src, dst, ss, rs, count):
        size = src.shape[0] // 16 * count
        return pltpu.make_async_remote_copy(
            src.at[pl.ds(0, size)], dst.at[pl.ds(0, size)], ss, rs,
            device_id={"sp": sp}, device_id_type=MESH,
        )

    all_blocks(ka, ka, kvs.at[0], kvr.at[0], 16).wait_recv()

    lam = lam_ref[sp]
    gain = gain_ref[pl.ds(sp, 1), :] * 0.8
    first = lax.broadcasted_iota(jnp.int32, (QB, VD), 1) < HD
    scale = HD ** (-0.5) * LOG2E

    def pair_of(step):
        return (sp // 2 + step) % STEPS

    def queries_arrive(step):
        for b in range(2):
            pltpu.make_async_remote_copy(
                q_ref.at[:, mine], qa.at[cols(2 * pair_of(step) + b), :],
                qs.at[2 * step + b], qr.at[2 * step + b],
                device_id={"sp": sp}, device_id_type=MESH,
            ).wait_recv()

    def scores(step, s1, s2):
        q = qa[rows_of(pair_of(step), QB), :]
        zero = jnp.zeros_like(q)
        q1 = jnp.where(first, q, zero)
        q2 = jnp.where(first, zero, q)
        dims = (((1,), (1,)), ((), ()))
        for c in range(SEQ // KC):
            k = ka[c * KC : (c + 1) * KC, :]
            at = pl.ds(c * KC, KC)
            s1[:, at] = lax.dot_general(q1, k, dims, preferred_element_type=F32)
            s2[:, at] = lax.dot_general(q2, k, dims, preferred_element_type=F32)

    def mixed(step, s1, s2):
        for r in range(QB // RB):
            at = pl.ds(r * RB, RB)
            a = s1[at, :]
            e1 = jnp.exp2((a - jnp.max(a, axis=1, keepdims=True)) * scale)
            l1 = jnp.sum(e1, axis=1, keepdims=True)
            b = s2[at, :]
            e2 = jnp.exp2((b - jnp.max(b, axis=1, keepdims=True)) * scale)
            l2 = jnp.sum(e2, axis=1, keepdims=True)
            maps[step, at, :] = (e1 - e2 * (lam * l1 / l2)).astype(BF16)
            sums[step, at, :] = l1

    def valued(step):
        out = jnp.dot(maps[step], va[...], preferred_element_type=F32)
        out = out / sums[step]
        out = out * lax.rsqrt(jnp.mean(out * out, axis=1, keepdims=True) + eps) * gain
        obuf[rows_of(pair_of(step), QB), :] = out.astype(BF16)

    def heads_leave(step):
        for b in range(2):
            to = 2 * pair_of(step) + b
            copy = pltpu.make_async_remote_copy(
                obuf.at[cols(to), :], att.at[:, mine], os_, or_.at[step],
                device_id={"sp": to}, device_id_type=MESH,
            )
            if step:
                copy.start()
            else:
                own = pltpu.make_async_copy(obuf.at[mine, :], att.at[:, mine], or_.at[0])
                pl.when(to != sp)(copy.start)
                pl.when(to == sp)(own.start)

    def pair(i, carry):
        step = 2 * i
        queries_arrive(step + 1)
        scores(step + 1, s1b, s2b)
        mixed(step, s1a, s2a)
        queries_arrive(step + 2)
        scores(step + 2, s1a, s2a)
        mixed(step + 1, s1b, s2b)
        return carry

    queries_arrive(0)
    scores(0, s1a, s2a)
    lax.fori_loop(0, HALF // 2, pair, 0)
    all_blocks(va, va, kvs.at[1], kvr.at[1], 16).wait_recv()
    for step in range(HALF, STEPS):
        now, later = ((s1a, s2a), (s1b, s2b))[:: 1 if step % 2 == 0 else -1]
        if step + 1 < STEPS:
            queries_arrive(step + 1)
            scores(step + 1, *later)
        mixed(step, *now)
        for done in (2 * (step - HALF), 2 * (step - HALF) + 1):
            valued(done)
            heads_leave(done)

    inputs[3].wait()
    loads[0].wait()
    for step in range(STEPS):
        all_blocks(obuf, obuf, os_, or_.at[step], 2).wait_recv()
        heads = rows_of((sp // 2 + STEPS - step) % STEPS, 2 * VD)
        for n in range(D // NC):
            at = slice(n * NC, (n + 1) * NC)
            part = jnp.dot(att[:, heads], wo[heads, at], preferred_element_type=F32)
            total[:, at] = part + total[:, at] if step else part

    squares = jnp.zeros((TOK, 1), F32)
    for n in range(D // NC):
        at = slice(n * NC, (n + 1) * NC)
        whole = (res_ref[:, at].astype(F32) + total[:, at]).astype(BF16)
        mid[:, at] = whole
        whole = whole.astype(F32)
        squares = squares + jnp.sum(whole * whole, axis=1, keepdims=True)
    inverse = lax.rsqrt(squares * (1.0 / D) + eps)
    for n in range(D // NC):
        at = slice(n * NC, (n + 1) * NC)
        x = (mid[:, at].astype(F32) * inverse * ffn_ref[:, at]).astype(BF16)
        picked = jnp.dot(onehot[...], x, preferred_element_type=F32).astype(BF16)
        xs[:, :, at] = picked.reshape(EXPERTS, CAP, NC)

    pl.semaphore_wait(ready, 15)
    peers = [peer_of(sp, off) for off in PEERS] + [sp]
    others = [[chip_core(dp, dx, dc) for dc in range(2)] for dx in range(4)]
    for g in range(4):
        for j, (dz, dy, dc) in enumerate(INNER):
            i = g * GROUP + j
            if (g, j) == (OWN_GROUP, OWN_AT):
                pltpu.make_async_copy(xs.at[expert], rx.at[i], dr.at[g]).start()
                continue
            to_sp, to_dp = peers[j // 2], others[(g + dz + dy) % 4][dc]
            pltpu.make_async_remote_copy(
                xs.at[to_sp * 8 + to_dp], rx.at[i], ds.at[g], dr.at[g],
                device_id={"sp": to_sp, "dp": to_dp}, device_id_type=MESH,
            ).start()
    for load in loads[1:]:
        load.wait()

    def whole_batch(src, dst, ss, rs, count):
        return pltpu.make_async_remote_copy(
            src.at[pl.ds(0, count)], dst.at[pl.ds(0, count)], ss, rs,
            device_id={"sp": sp}, device_id_type=MESH,
        )

    homes = [peer_of(sp, minus(off)) for off in PEERS] + [sp]

    def batch(g, carry):
        at = rows_of(g, GROUP)
        whole_batch(xs, rx, ds.at[g], dr.at[g], GROUP).wait_recv()
        x = rx[at].reshape(GROUP * CAP, D)
        for n in range(FF // 256):
            w = slice(n * 256, (n + 1) * 256)
            gate = jnp.dot(x, wg[:, w], preferred_element_type=F32)
            up = jnp.dot(x, wu[:, w], preferred_element_type=F32)
            hid[:, w] = (gate / (1.0 + jnp.exp(-gate)) * up).astype(BF16)
        h = hid[...]
        for n in range(D // NC):
            w = slice(n * NC, (n + 1) * NC)
            y = jnp.dot(h, wd[:, w], preferred_element_type=F32).astype(BF16)
            yx[at, :, w] = y.reshape(GROUP, CAP, NC)
        back_to = [[chip_core(dp, (8 - g - turn) % 4, dc) for dc in range(2)] for turn in range(4)]
        for j, (dz, dy, dc) in enumerate(INNER):
            i = g * GROUP + j
            back = pltpu.make_async_remote_copy(
                yx.at[i], ret.at[expert], es.at[g], er.at[g],
                device_id={"sp": homes[j // 2], "dp": back_to[(dz + dy) % 4][dc]},
                device_id_type=MESH,
            )
            if j == OWN_AT:
                own = pltpu.make_async_copy(yx.at[i], ret.at[expert], er.at[g])
                pl.when(g != OWN_GROUP)(back.start)
                pl.when(g == OWN_GROUP)(own.start)
            else:
                back.start()
        return carry

    lax.fori_loop(0, 4, batch, 0)

    for g in range(4):
        whole_batch(yx, ret, es.at[g], er.at[g], GROUP).wait_recv()
    leaving = []
    for n in range(D // NC):
        at = slice(n * NC, (n + 1) * NC)
        r = ret[:, :, at].reshape(SLOTS, NC)
        dims = (((0,), (0,)), ((), ()))
        moe = lax.dot_general(chigh[...], r, dims, preferred_element_type=F32)
        moe = moe + lax.dot_general(clow[...], r, dims, preferred_element_type=F32)
        out[:, at] = (mid[:, at].astype(F32) + moe).astype(BF16)
        leave = pltpu.make_async_copy(out.at[:, at], out_hbm.at[:, at], outsem.at[n])
        leave.start()
        leaving.append(leave)

    all_blocks(ka, ka, kvs.at[0], kvr.at[0], 15).wait_send()
    all_blocks(va, va, kvs.at[1], kvr.at[1], 15).wait_send()
    all_blocks(obuf, obuf, os_, or_, 15).wait_send()
    for g in range(4):
        count = GROUP - (g == OWN_GROUP)
        whole_batch(xs, rx, ds.at[g], dr.at[g], count).wait_send()
        whole_batch(yx, ret, es.at[g], er.at[g], count).wait_send()
    for i in range(STEPS):
        for b in range(2):
            to, copy = query_copy(i, b)
            if i == 0:
                pl.when(to != sp)(copy.wait_send)
            else:
                copy.wait_send()
    for leave in leaving:
        leave.wait()


def on_device(
    residual, query_maps, key_maps, value_rows, lambdas, head_gain, out_weight, ffn_gain,
    routes, route_weights, expert_gate, expert_up, expert_down,
):
    vmem = pl.BlockSpec(memory_space=pltpu.VMEM)
    smem = pl.BlockSpec(memory_space=pltpu.SMEM)
    hbm = pl.BlockSpec(memory_space=pl.ANY)
    score = pltpu.VMEM((QB, SEQ), F32)
    rows = pltpu.VMEM((SEQ, VD), BF16)
    tokens = pltpu.VMEM((TOK, D), BF16)
    table = pltpu.VMEM((SLOTS, TOK), BF16)
    slots = pltpu.VMEM((EXPERTS, CAP, D), BF16)
    sem = pltpu.SemaphoreType.DMA
    out = pl.pallas_call(
        layer_kernel,
        out_shape=jax.ShapeDtypeStruct((TOK, D), BF16),
        in_specs=[hbm] * 4 + [smem] + [vmem] * 4 + [hbm] * 4,
        out_specs=hbm,
        scratch_shapes=[tokens] * 4 + [rows, rows, rows, score, score, score, score,
                        pltpu.VMEM((STEPS, QB, SEQ), BF16), pltpu.VMEM((STEPS, QB, 1), F32), rows, tokens,
                        pltpu.VMEM((TOK, D), F32), tokens, tokens,
                        table, table, table,
                        pltpu.VMEM((D, D), BF16), pltpu.VMEM((D, FF), BF16),
                        pltpu.VMEM((D, FF), BF16), pltpu.VMEM((FF, D), BF16),
                        slots, slots, pltpu.VMEM((GROUP * CAP, FF), BF16), slots, slots]
        + [sem((2,)), sem((2,)), sem((16,)), sem((16,)), sem, sem((STEPS,))] + [sem((4,))] * 7
        + [pltpu.SemaphoreType.REGULAR],
        compiler_params=pltpu.CompilerParams(
            collective_id=0, has_side_effects=True, vmem_limit_bytes=60 * 2**20
        ),
        name="layer",
    )(
        query_maps[0], key_maps[0], value_rows[0], residual[0], lambdas,
        head_gain.reshape(HEADS, VD), ffn_gain.reshape(1, D), routes[0].T, route_weights[0].T,
        out_weight, expert_gate[0], expert_up[0], expert_down[0],
    )
    return out[None]


def solution(mesh):
    tokens = P("dp", "sp", None)
    experts = P(("sp", "dp"), None, None)
    placed = (tokens,) * 4 + (P(),) * 4 + (tokens,) * 2 + (experts,) * 3
    return jax.shard_map(
        on_device, mesh=mesh, in_specs=placed, out_specs=tokens, check_vma=False
    )
```

```python
import jax
import jax.numpy as jnp
from jax import lax
from jax.experimental import pallas as pl
from jax.experimental.pallas import tpu as pltpu
from jax.sharding import PartitionSpec as P

D = 2048
HEADS = 16
HD = 64
VD = 128
FF = 1024
TOK = 128
SEQ = 2048
EXPERTS = 128
CAP = 4
SLOTS = EXPERTS * CAP
QB = 256
STEPS = SEQ // QB
HALF = 6
KC = 256
RB = 16
NC = 512
GROUP = 32
MESH = pl.DeviceIdType.MESH
eps = 1e-06
LOG2E = 1.4426950408889634
F32 = jnp.float32
BF16 = jnp.bfloat16
NEAR = {0: 0, 1: 1, 2: 2, 3: 1}
PEERS = sorted(
    [(a, b) for a in range(4) for b in range(4) if (a, b) != (0, 0)],
    key=lambda o: -(NEAR[o[0]] + NEAR[o[1]]),
)
INNER = [(a, b, c) for a, b in PEERS + [(0, 0)] for c in (1, 0)]
OWN_GROUP, OWN_AT = 0, INNER.index((0, 0, 0))


def peer_of(me, off):
    return ((me // 4 + off[0]) % 4) * 4 + (me % 4 + off[1]) % 4


def minus(off):
    return tuple((4 - o) % 4 for o in off)


def chip_core(me, dx, dc):
    return ((me // 2 + dx) % 4) * 2 + (me % 2 + dc) % 2


def cols(block):
    return pl.ds(pl.multiple_of(block * VD, VD), VD)


def rows_of(step, size):
    return pl.ds(pl.multiple_of(step * size, size), size)


def layer_kernel(
    q_hbm, k_hbm, v_hbm, res_hbm, lam_ref, gain_ref, ffn_ref, route_ref, weight_ref,
    wo_hbm, wg_hbm, wu_hbm, wd_hbm,
    out_ref,
    q_ref, k_ref, v_ref, res_ref,
    qa, ka, va, s1a, s2a, s1b, s2b, maps, sums, obuf, att, total, mid, onehot, chigh, clow,
    wo, wg, wu, wd, xs, rx, hid, yx, ret,
    kvs, kvr, qs, qr, os_, or_, ds, dr, es, er, insem, wsem, smallsem, ready,
):
    sp = lax.axis_index("sp")
    dp = lax.axis_index("dp")
    expert = sp * 8 + dp
    barrier = pltpu.get_barrier_semaphore()
    for off in PEERS:
        pl.semaphore_signal(barrier, inc=1, device_id={"sp": peer_of(sp, off)}, device_id_type=MESH)
    for i in range(1, 8):
        to = chip_core(dp, i // 2, i % 2)
        pl.semaphore_signal(barrier, inc=1, device_id={"dp": to}, device_id_type=MESH)
    inputs = []
    for i, (src, dst) in enumerate(((k_hbm, k_ref), (v_hbm, v_ref), (q_hbm, q_ref), (res_hbm, res_ref))):
        load = pltpu.make_async_copy(src, dst, insem.at[i])
        load.start()
        inputs.append(load)
    pl.semaphore_wait(barrier, 22)
    for off in PEERS:
        pl.semaphore_signal(ready, inc=1, device_id={"sp": peer_of(sp, off)}, device_id_type=MESH)

    mine = cols(sp)

    def rows_leave(n, src, dst):
        inputs[n].wait()
        for off in PEERS:
            to = peer_of(sp, off)
            pltpu.make_async_remote_copy(
                src.at[:, cols(to)], dst.at[mine, :], kvs.at[n], kvr.at[n],
                device_id={"sp": to}, device_id_type=MESH,
            ).start()
        pltpu.make_async_copy(src.at[:, mine], dst.at[mine, :], kvr.at[n]).start()

    def query_copy(i, b):
        to = 2 * ((sp // 2 + 8 - i) % 8) + b
        return to, pltpu.make_async_remote_copy(
            q_ref.at[:, cols(to)], qa.at[mine, :], qs.at[2 * i + b], qr.at[2 * i + sp % 2],
            device_id={"sp": to}, device_id_type=MESH,
        )

    def queries_leave(steps):
        for i in steps:
            for b in range(2):
                to, copy = query_copy(i, b)
                if i == 0:
                    pl.when(to != sp)(copy.start)
                else:
                    copy.start()

    rows_leave(0, k_ref, ka)
    inputs[2].wait()
    pltpu.make_async_copy(q_ref.at[:, mine], qa.at[mine, :], qr.at[sp % 2]).start()
    queries_leave(range(HALF))
    rows_leave(1, v_ref, va)
    queries_leave(range(HALF, STEPS))
    loads = []
    for i, (src, dst) in enumerate(((wo_hbm, wo), (wg_hbm, wg), (wu_hbm, wu), (wd_hbm, wd))):
        load = pltpu.make_async_copy(src, dst, wsem.at[i])
        load.start()
        loads.append(load)

    names = lax.broadcasted_iota(jnp.int32, (EXPERTS, TOK), 0)
    earlier = lax.broadcasted_iota(jnp.int32, (TOK, TOK), 0) < lax.broadcasted_iota(jnp.int32, (TOK, TOK), 1)
    earlier = jnp.where(earlier, 1.0, 0.0).astype(BF16)
    slots = lax.broadcasted_iota(jnp.int32, (SLOTS, TOK), 0).astype(F32)
    ahead = jnp.zeros((EXPERTS, 1), F32)
    marks = jnp.zeros((SLOTS, TOK), F32)
    combine = jnp.zeros((SLOTS, TOK), F32)
    for k in range(2):
        named = route_ref[k : k + 1, :]
        mark = jnp.where(named == names, 1.0, 0.0)
        before = jnp.dot(mark.astype(BF16), earlier, preferred_element_type=F32) + ahead
        rank = jnp.sum(before * mark, axis=0, keepdims=True)
        here = named.astype(F32) * CAP + rank == slots
        marks = jnp.where(here, 1.0, marks)
        combine = jnp.where(here, weight_ref[k : k + 1, :], combine)
        ahead = ahead + jnp.sum(mark, axis=1, keepdims=True)
    onehot[...] = marks.astype(BF16)
    high = combine.astype(BF16)
    chigh[...] = high
    clow[...] = (combine - high.astype(F32)).astype(BF16)

    def all_blocks(src, dst, ss, rs, count):
        size = src.shape[0] // 16 * count
        return pltpu.make_async_remote_copy(
            src.at[pl.ds(0, size)], dst.at[pl.ds(0, size)], ss, rs,
            device_id={"sp": sp}, device_id_type=MESH,
        )

    all_blocks(ka, ka, kvs.at[0], kvr.at[0], 16).wait_recv()

    lam = lam_ref[sp]
    gain = gain_ref[pl.ds(sp, 1), :] * 0.8
    first = lax.broadcasted_iota(jnp.int32, (QB, VD), 1) < HD
    scale = HD ** (-0.5) * LOG2E

    def pair_of(step):
        return (sp // 2 + step) % STEPS

    def queries_arrive(step):
        for b in range(2):
            pltpu.make_async_remote_copy(
                q_ref.at[:, mine], qa.at[cols(2 * pair_of(step) + b), :],
                qs.at[2 * step + b], qr.at[2 * step + b],
                device_id={"sp": sp}, device_id_type=MESH,
            ).wait_recv()

    def scores(step, s1, s2):
        q = qa[rows_of(pair_of(step), QB), :]
        zero = jnp.zeros_like(q)
        q1 = jnp.where(first, q, zero)
        q2 = jnp.where(first, zero, q)
        dims = (((1,), (1,)), ((), ()))
        for c in range(SEQ // KC):
            k = ka[c * KC : (c + 1) * KC, :]
            at = pl.ds(c * KC, KC)
            s1[:, at] = lax.dot_general(q1, k, dims, preferred_element_type=F32)
            s2[:, at] = lax.dot_general(q2, k, dims, preferred_element_type=F32)

    def mixed(step, s1, s2):
        for r in range(QB // RB):
            at = pl.ds(r * RB, RB)
            a = s1[at, :]
            e1 = jnp.exp2((a - jnp.max(a, axis=1, keepdims=True)) * scale)
            l1 = jnp.sum(e1, axis=1, keepdims=True)
            b = s2[at, :]
            e2 = jnp.exp2((b - jnp.max(b, axis=1, keepdims=True)) * scale)
            l2 = jnp.sum(e2, axis=1, keepdims=True)
            maps[step, at, :] = (e1 - e2 * (lam * l1 / l2)).astype(BF16)
            sums[step, at, :] = l1

    def valued(step):
        out = jnp.dot(maps[step], va[...], preferred_element_type=F32)
        out = out / sums[step]
        out = out * lax.rsqrt(jnp.mean(out * out, axis=1, keepdims=True) + eps) * gain
        obuf[rows_of(pair_of(step), QB), :] = out.astype(BF16)

    def heads_leave(step):
        for b in range(2):
            to = 2 * pair_of(step) + b
            copy = pltpu.make_async_remote_copy(
                obuf.at[cols(to), :], att.at[:, mine], os_, or_.at[step],
                device_id={"sp": to}, device_id_type=MESH,
            )
            if step:
                copy.start()
            else:
                own = pltpu.make_async_copy(obuf.at[mine, :], att.at[:, mine], or_.at[0])
                pl.when(to != sp)(copy.start)
                pl.when(to == sp)(own.start)

    def pair(i, carry):
        step = 2 * i
        queries_arrive(step + 1)
        scores(step + 1, s1b, s2b)
        mixed(step, s1a, s2a)
        queries_arrive(step + 2)
        scores(step + 2, s1a, s2a)
        mixed(step + 1, s1b, s2b)
        return carry

    queries_arrive(0)
    scores(0, s1a, s2a)
    lax.fori_loop(0, HALF // 2, pair, 0)
    all_blocks(va, va, kvs.at[1], kvr.at[1], 16).wait_recv()
    for step in range(HALF, STEPS):
        now, later = ((s1a, s2a), (s1b, s2b))[:: 1 if step % 2 == 0 else -1]
        if step + 1 < STEPS:
            queries_arrive(step + 1)
            scores(step + 1, *later)
        mixed(step, *now)
        for done in range((step - HALF) * STEPS // (STEPS - HALF), (step - HALF + 1) * STEPS // (STEPS - HALF)):
            valued(done)
            heads_leave(done)

    inputs[3].wait()
    loads[0].wait()
    for step in range(STEPS):
        all_blocks(obuf, obuf, os_, or_.at[step], 2).wait_recv()
        heads = rows_of((sp // 2 + STEPS - step) % STEPS, 2 * VD)
        for n in range(D // NC):
            at = slice(n * NC, (n + 1) * NC)
            part = jnp.dot(att[:, heads], wo[heads, at], preferred_element_type=F32)
            total[:, at] = part + total[:, at] if step else part

    squares = jnp.zeros((TOK, 1), F32)
    for n in range(D // NC):
        at = slice(n * NC, (n + 1) * NC)
        whole = (res_ref[:, at].astype(F32) + total[:, at]).astype(BF16)
        mid[:, at] = whole
        whole = whole.astype(F32)
        squares = squares + jnp.sum(whole * whole, axis=1, keepdims=True)
    inverse = lax.rsqrt(squares * (1.0 / D) + eps)
    for n in range(D // NC):
        at = slice(n * NC, (n + 1) * NC)
        x = (mid[:, at].astype(F32) * inverse * ffn_ref[:, at]).astype(BF16)
        picked = jnp.dot(onehot[...], x, preferred_element_type=F32).astype(BF16)
        xs[:, :, at] = picked.reshape(EXPERTS, CAP, NC)

    pl.semaphore_wait(ready, 15)
    peers = [peer_of(sp, off) for off in PEERS] + [sp]
    others = [[chip_core(dp, dx, dc) for dc in range(2)] for dx in range(4)]
    for g in range(4):
        for j, (dz, dy, dc) in enumerate(INNER):
            i = g * GROUP + j
            if (g, j) == (OWN_GROUP, OWN_AT):
                pltpu.make_async_copy(xs.at[expert], rx.at[i], dr.at[g]).start()
                continue
            to_sp, to_dp = peers[j // 2], others[(g + dz + dy) % 4][dc]
            pltpu.make_async_remote_copy(
                xs.at[to_sp * 8 + to_dp], rx.at[i], ds.at[g], dr.at[g],
                device_id={"sp": to_sp, "dp": to_dp}, device_id_type=MESH,
            ).start()
    for load in loads[1:]:
        load.wait()

    def whole_batch(src, dst, ss, rs, count):
        return pltpu.make_async_remote_copy(
            src.at[pl.ds(0, count)], dst.at[pl.ds(0, count)], ss, rs,
            device_id={"sp": sp}, device_id_type=MESH,
        )

    homes = [peer_of(sp, minus(off)) for off in PEERS] + [sp]

    def arrive(g):
        whole_batch(xs, rx, ds.at[g], dr.at[g], GROUP).wait_recv()

    def work(g):
        at = rows_of(g, GROUP)
        x = rx[at].reshape(GROUP * CAP, D)
        for n in range(FF // 256):
            w = slice(n * 256, (n + 1) * 256)
            gate = jnp.dot(x, wg[:, w], preferred_element_type=F32)
            up = jnp.dot(x, wu[:, w], preferred_element_type=F32)
            hid[:, w] = (gate / (1.0 + jnp.exp(-gate)) * up).astype(BF16)
        h = hid[...]
        for n in range(D // NC):
            w = slice(n * NC, (n + 1) * NC)
            y = jnp.dot(h, wd[:, w], preferred_element_type=F32).astype(BF16)
            yx[at, :, w] = y.reshape(GROUP, CAP, NC)

    def give_back(g):
        back_to = [[chip_core(dp, (8 - g - turn) % 4, dc) for dc in range(2)] for turn in range(4)]
        for j, (dz, dy, dc) in enumerate(INNER):
            i = g * GROUP + j
            back = pltpu.make_async_remote_copy(
                yx.at[i], ret.at[expert], es.at[g], er.at[g],
                device_id={"sp": homes[j // 2], "dp": back_to[(dz + dy) % 4][dc]},
                device_id_type=MESH,
            )
            if j == OWN_AT:
                own = pltpu.make_async_copy(yx.at[i], ret.at[expert], er.at[g])
                pl.when(g != OWN_GROUP)(back.start)
                pl.when(g == OWN_GROUP)(own.start)
            else:
                back.start()

    def early(g, carry):
        arrive(g)
        work(g)
        return carry

    def late(g, carry):
        give_back(g)
        return carry

    lax.fori_loop(0, 3, early, 0)
    arrive(3)
    lax.fori_loop(0, 3, late, 0)

    def last(g, carry):
        work(g)
        give_back(g)
        return carry

    lax.fori_loop(3, 4, last, 0)

    for g in range(4):
        whole_batch(yx, ret, es.at[g], er.at[g], GROUP).wait_recv()
    for n in range(D // NC):
        at = slice(n * NC, (n + 1) * NC)
        r = ret[:, :, at].reshape(SLOTS, NC)
        dims = (((0,), (0,)), ((), ()))
        moe = lax.dot_general(chigh[...], r, dims, preferred_element_type=F32)
        moe = moe + lax.dot_general(clow[...], r, dims, preferred_element_type=F32)
        out_ref[:, at] = (mid[:, at].astype(F32) + moe).astype(BF16)

    all_blocks(ka, ka, kvs.at[0], kvr.at[0], 15).wait_send()
    all_blocks(va, va, kvs.at[1], kvr.at[1], 15).wait_send()
    all_blocks(obuf, obuf, os_, or_, 15).wait_send()
    for g in range(4):
        count = GROUP - (g == OWN_GROUP)
        whole_batch(xs, rx, ds.at[g], dr.at[g], count).wait_send()
        whole_batch(yx, ret, es.at[g], er.at[g], count).wait_send()
    for i in range(STEPS):
        for b in range(2):
            to, copy = query_copy(i, b)
            if i == 0:
                pl.when(to != sp)(copy.wait_send)
            else:
                copy.wait_send()


def on_device(
    residual, query_maps, key_maps, value_rows, lambdas, head_gain, out_weight, ffn_gain,
    routes, route_weights, expert_gate, expert_up, expert_down,
):
    vmem = pl.BlockSpec(memory_space=pltpu.VMEM)
    smem = pl.BlockSpec(memory_space=pltpu.SMEM)
    hbm = pl.BlockSpec(memory_space=pl.ANY)
    score = pltpu.VMEM((QB, SEQ), F32)
    rows = pltpu.VMEM((SEQ, VD), BF16)
    tokens = pltpu.VMEM((TOK, D), BF16)
    table = pltpu.VMEM((SLOTS, TOK), BF16)
    slots = pltpu.VMEM((EXPERTS, CAP, D), BF16)
    sem = pltpu.SemaphoreType.DMA
    out = pl.pallas_call(
        layer_kernel,
        out_shape=pltpu.VMEM((TOK, D), BF16),
        in_specs=[hbm] * 4 + [smem] + [vmem] * 4 + [hbm] * 4,
        out_specs=vmem,
        scratch_shapes=[tokens] * 4 + [rows, rows, rows, score, score, score, score,
                        pltpu.VMEM((STEPS, QB, SEQ), BF16), pltpu.VMEM((STEPS, QB, 1), F32), rows, tokens,
                        pltpu.VMEM((TOK, D), F32), tokens,
                        table, table, table,
                        pltpu.VMEM((D, D), BF16), pltpu.VMEM((D, FF), BF16),
                        pltpu.VMEM((D, FF), BF16), pltpu.VMEM((FF, D), BF16),
                        slots, slots, pltpu.VMEM((GROUP * CAP, FF), BF16), slots, slots]
        + [sem((2,)), sem((2,)), sem((16,)), sem((16,)), sem, sem((STEPS,))] + [sem((4,))] * 7
        + [pltpu.SemaphoreType.REGULAR],
        compiler_params=pltpu.CompilerParams(
            collective_id=0, has_side_effects=True, vmem_limit_bytes=60 * 2**20
        ),
        name="layer",
    )(
        query_maps[0], key_maps[0], value_rows[0], residual[0], lambdas,
        head_gain.reshape(HEADS, VD), ffn_gain.reshape(1, D), routes[0].T, route_weights[0].T,
        out_weight, expert_gate[0], expert_up[0], expert_down[0],
    )
    return out[None]


def solution(mesh):
    tokens = P("dp", "sp", None)
    experts = P(("sp", "dp"), None, None)
    placed = (tokens,) * 4 + (P(),) * 4 + (tokens,) * 2 + (experts,) * 3
    return jax.shard_map(
        on_device, mesh=mesh, in_specs=placed, out_specs=tokens, check_vma=False
    )
```

```python
import jax
import jax.numpy as jnp
from jax import lax
from jax.experimental import pallas as pl
from jax.experimental.pallas import tpu as pltpu
from jax.sharding import PartitionSpec as P

D = 2048
HEADS = 16
HD = 64
VD = 128
FF = 1024
TOK = 128
SEQ = 2048
EXPERTS = 128
CAP = 4
SLOTS = EXPERTS * CAP
QB = 256
STEPS = SEQ // QB
HALF = 6
KC = 256
RB = 16
NC = 512
GROUP = 32
MESH = pl.DeviceIdType.MESH
eps = 1e-06
LOG2E = 1.4426950408889634
F32 = jnp.float32
BF16 = jnp.bfloat16
NEAR = {0: 0, 1: 1, 2: 2, 3: 1}
PEERS = sorted(
    [(a, b) for a in range(4) for b in range(4) if (a, b) != (0, 0)],
    key=lambda o: -(NEAR[o[0]] + NEAR[o[1]]),
)
INNER = [(a, b, c) for a, b in PEERS + [(0, 0)] for c in (1, 0)]
OWN_GROUP, OWN_AT = 0, INNER.index((0, 0, 0))


def peer_of(me, off):
    return ((me // 4 + off[0]) % 4) * 4 + (me % 4 + off[1]) % 4


def minus(off):
    return tuple((4 - o) % 4 for o in off)


def chip_core(me, dx, dc):
    return ((me // 2 + dx) % 4) * 2 + (me % 2 + dc) % 2


def cols(block):
    return pl.ds(pl.multiple_of(block * VD, VD), VD)


def rows_of(step, size):
    return pl.ds(pl.multiple_of(step * size, size), size)


def layer_kernel(
    q_hbm, k_hbm, v_hbm, res_hbm, lam_ref, gain_ref, ffn_ref, route_ref, weight_ref,
    wo_hbm, wg_hbm, wu_hbm, wd_hbm,
    out_ref,
    q_ref, k_ref, v_ref, res_ref,
    qa, ka, va, s1a, s2a, s1b, s2b, maps, sums, obuf, att, total, mid, onehot, chigh, clow,
    wo, wg, wu, wd, xs, rx, hid, yx, ret,
    kvs, kvr, qs, qr, os_, or_, ds, dr, es, er, insem, wsem, smallsem, ready,
):
    sp = lax.axis_index("sp")
    dp = lax.axis_index("dp")
    expert = sp * 8 + dp
    barrier = pltpu.get_barrier_semaphore()
    for off in PEERS:
        pl.semaphore_signal(barrier, inc=1, device_id={"sp": peer_of(sp, off)}, device_id_type=MESH)
    for i in range(1, 8):
        to = chip_core(dp, i // 2, i % 2)
        pl.semaphore_signal(barrier, inc=1, device_id={"dp": to}, device_id_type=MESH)
    inputs = []
    for i, (src, dst) in enumerate(((k_hbm, k_ref), (v_hbm, v_ref), (q_hbm, q_ref), (res_hbm, res_ref))):
        load = pltpu.make_async_copy(src, dst, insem.at[i])
        load.start()
        inputs.append(load)
    pl.semaphore_wait(barrier, 22)
    for off in PEERS:
        pl.semaphore_signal(ready, inc=1, device_id={"sp": peer_of(sp, off)}, device_id_type=MESH)

    mine = cols(sp)

    def rows_leave(n, src, dst):
        inputs[n].wait()
        for off in PEERS:
            to = peer_of(sp, off)
            pltpu.make_async_remote_copy(
                src.at[:, cols(to)], dst.at[mine, :], kvs.at[n], kvr.at[n],
                device_id={"sp": to}, device_id_type=MESH,
            ).start()
        pltpu.make_async_copy(src.at[:, mine], dst.at[mine, :], kvr.at[n]).start()

    def query_copy(i, b):
        to = 2 * ((sp // 2 + 8 - i) % 8) + b
        return to, pltpu.make_async_remote_copy(
            q_ref.at[:, cols(to)], qa.at[mine, :], qs.at[2 * i + b], qr.at[2 * i + sp % 2],
            device_id={"sp": to}, device_id_type=MESH,
        )

    def queries_leave(steps):
        for i in steps:
            for b in range(2):
                to, copy = query_copy(i, b)
                if i == 0:
                    pl.when(to != sp)(copy.start)
                else:
                    copy.start()

    rows_leave(0, k_ref, ka)
    inputs[2].wait()
    pltpu.make_async_copy(q_ref.at[:, mine], qa.at[mine, :], qr.at[sp % 2]).start()
    queries_leave(range(HALF))
    rows_leave(1, v_ref, va)
    queries_leave(range(HALF, STEPS))
    loads = []
    for i, (src, dst) in enumerate(((wo_hbm, wo), (wg_hbm, wg), (wu_hbm, wu), (wd_hbm, wd))):
        load = pltpu.make_async_copy(src, dst, wsem.at[i])
        load.start()
        loads.append(load)

    names = lax.broadcasted_iota(jnp.int32, (EXPERTS, TOK), 0)
    earlier = lax.broadcasted_iota(jnp.int32, (TOK, TOK), 0) < lax.broadcasted_iota(jnp.int32, (TOK, TOK), 1)
    earlier = jnp.where(earlier, 1.0, 0.0).astype(BF16)
    slots = lax.broadcasted_iota(jnp.int32, (SLOTS, TOK), 0).astype(F32)
    ahead = jnp.zeros((EXPERTS, 1), F32)
    marks = jnp.zeros((SLOTS, TOK), F32)
    combine = jnp.zeros((SLOTS, TOK), F32)
    for k in range(2):
        named = route_ref[k : k + 1, :]
        mark = jnp.where(named == names, 1.0, 0.0)
        before = jnp.dot(mark.astype(BF16), earlier, preferred_element_type=F32) + ahead
        rank = jnp.sum(before * mark, axis=0, keepdims=True)
        here = named.astype(F32) * CAP + rank == slots
        marks = jnp.where(here, 1.0, marks)
        combine = jnp.where(here, weight_ref[k : k + 1, :], combine)
        ahead = ahead + jnp.sum(mark, axis=1, keepdims=True)
    onehot[...] = marks.astype(BF16)
    high = combine.astype(BF16)
    chigh[...] = high
    clow[...] = (combine - high.astype(F32)).astype(BF16)

    def all_blocks(src, dst, ss, rs, count):
        size = src.shape[0] // 16 * count
        return pltpu.make_async_remote_copy(
            src.at[pl.ds(0, size)], dst.at[pl.ds(0, size)], ss, rs,
            device_id={"sp": sp}, device_id_type=MESH,
        )

    all_blocks(ka, ka, kvs.at[0], kvr.at[0], 16).wait_recv()

    lam = lam_ref[sp]
    gain = gain_ref[pl.ds(sp, 1), :] * 0.8
    first = lax.broadcasted_iota(jnp.int32, (QB, VD), 1) < HD
    scale = HD ** (-0.5) * LOG2E

    def pair_of(step):
        return (sp // 2 + step) % STEPS

    def queries_arrive(step):
        for b in range(2):
            pltpu.make_async_remote_copy(
                q_ref.at[:, mine], qa.at[cols(2 * pair_of(step) + b), :],
                qs.at[2 * step + b], qr.at[2 * step + b],
                device_id={"sp": sp}, device_id_type=MESH,
            ).wait_recv()

    def scores(step, s1, s2):
        q = qa[rows_of(pair_of(step), QB), :]
        zero = jnp.zeros_like(q)
        q1 = jnp.where(first, q, zero)
        q2 = jnp.where(first, zero, q)
        dims = (((1,), (1,)), ((), ()))
        for c in range(SEQ // KC):
            k = ka[c * KC : (c + 1) * KC, :]
            at = pl.ds(c * KC, KC)
            s1[:, at] = lax.dot_general(q1, k, dims, preferred_element_type=F32)
            s2[:, at] = lax.dot_general(q2, k, dims, preferred_element_type=F32)

    def mixed(step, s1, s2):
        for r in range(QB // RB):
            at = pl.ds(r * RB, RB)
            a = s1[at, :]
            e1 = jnp.exp2((a - jnp.max(a, axis=1, keepdims=True)) * scale)
            l1 = jnp.sum(e1, axis=1, keepdims=True)
            b = s2[at, :]
            e2 = jnp.exp2((b - jnp.max(b, axis=1, keepdims=True)) * scale)
            l2 = jnp.sum(e2, axis=1, keepdims=True)
            maps[step, at, :] = (e1 - e2 * (lam * l1 / l2)).astype(BF16)
            sums[step, at, :] = l1

    def valued(step):
        out = jnp.dot(maps[step], va[...], preferred_element_type=F32)
        out = out / sums[step]
        out = out * lax.rsqrt(jnp.mean(out * out, axis=1, keepdims=True) + eps) * gain
        obuf[rows_of(pair_of(step), QB), :] = out.astype(BF16)

    def heads_leave(step):
        for b in range(2):
            to = 2 * pair_of(step) + b
            copy = pltpu.make_async_remote_copy(
                obuf.at[cols(to), :], att.at[:, mine], os_, or_.at[step],
                device_id={"sp": to}, device_id_type=MESH,
            )
            if step:
                copy.start()
            else:
                own = pltpu.make_async_copy(obuf.at[mine, :], att.at[:, mine], or_.at[0])
                pl.when(to != sp)(copy.start)
                pl.when(to == sp)(own.start)

    def pair(i, carry):
        step = 2 * i
        queries_arrive(step + 1)
        scores(step + 1, s1b, s2b)
        mixed(step, s1a, s2a)
        queries_arrive(step + 2)
        scores(step + 2, s1a, s2a)
        mixed(step + 1, s1b, s2b)
        return carry

    queries_arrive(0)
    scores(0, s1a, s2a)
    lax.fori_loop(0, HALF // 2, pair, 0)
    all_blocks(va, va, kvs.at[1], kvr.at[1], 16).wait_recv()
    for step in range(HALF, STEPS):
        now, later = ((s1a, s2a), (s1b, s2b))[:: 1 if step % 2 == 0 else -1]
        if step + 1 < STEPS:
            queries_arrive(step + 1)
            scores(step + 1, *later)
        mixed(step, *now)
        for done in range((step - HALF) * STEPS // (STEPS - HALF), (step - HALF + 1) * STEPS // (STEPS - HALF)):
            valued(done)
            heads_leave(done)

    inputs[3].wait()
    loads[0].wait()
    for step in range(STEPS):
        all_blocks(obuf, obuf, os_, or_.at[step], 2).wait_recv()
        heads = rows_of((sp // 2 + STEPS - step) % STEPS, 2 * VD)
        for n in range(D // NC):
            at = slice(n * NC, (n + 1) * NC)
            part = jnp.dot(att[:, heads], wo[heads, at], preferred_element_type=F32)
            total[:, at] = part + total[:, at] if step else part

    squares = jnp.zeros((TOK, 1), F32)
    for n in range(D // NC):
        at = slice(n * NC, (n + 1) * NC)
        whole = (res_ref[:, at].astype(F32) + total[:, at]).astype(BF16)
        mid[:, at] = whole
        whole = whole.astype(F32)
        squares = squares + jnp.sum(whole * whole, axis=1, keepdims=True)
    inverse = lax.rsqrt(squares * (1.0 / D) + eps)
    for n in range(D // NC):
        at = slice(n * NC, (n + 1) * NC)
        x = (mid[:, at].astype(F32) * inverse * ffn_ref[:, at]).astype(BF16)
        picked = jnp.dot(onehot[...], x, preferred_element_type=F32).astype(BF16)
        xs[:, :, at] = picked.reshape(EXPERTS, CAP, NC)

    pl.semaphore_wait(ready, 15)
    peers = [peer_of(sp, off) for off in PEERS] + [sp]
    others = [[chip_core(dp, dx, dc) for dc in range(2)] for dx in range(4)]
    for g in range(4):
        for j, (dz, dy, dc) in enumerate(INNER):
            i = g * GROUP + j
            if (g, j) == (OWN_GROUP, OWN_AT):
                pltpu.make_async_copy(xs.at[expert], rx.at[i], dr.at[g]).start()
                continue
            to_sp, to_dp = peers[j // 2], others[(g + dz + dy) % 4][dc]
            pltpu.make_async_remote_copy(
                xs.at[to_sp * 8 + to_dp], rx.at[i], ds.at[g], dr.at[g],
                device_id={"sp": to_sp, "dp": to_dp}, device_id_type=MESH,
            ).start()
    for load in loads[1:]:
        load.wait()

    def whole_batch(src, dst, ss, rs, count):
        return pltpu.make_async_remote_copy(
            src.at[pl.ds(0, count)], dst.at[pl.ds(0, count)], ss, rs,
            device_id={"sp": sp}, device_id_type=MESH,
        )

    homes = [peer_of(sp, minus(off)) for off in PEERS] + [sp]

    def arrive(g):
        whole_batch(xs, rx, ds.at[g], dr.at[g], GROUP).wait_recv()

    def work(g):
        at = rows_of(g, GROUP)
        x = rx[at].reshape(GROUP * CAP, D)
        for n in range(FF // 256):
            w = slice(n * 256, (n + 1) * 256)
            gate = jnp.dot(x, wg[:, w], preferred_element_type=F32)
            up = jnp.dot(x, wu[:, w], preferred_element_type=F32)
            hid[:, w] = (gate / (1.0 + jnp.exp(-gate)) * up).astype(BF16)
        h = hid[...]
        for n in range(D // NC):
            w = slice(n * NC, (n + 1) * NC)
            y = jnp.dot(h, wd[:, w], preferred_element_type=F32).astype(BF16)
            yx[at, :, w] = y.reshape(GROUP, CAP, NC)

    def give_back(g):
        back_to = [[chip_core(dp, (8 - g - turn) % 4, dc) for dc in range(2)] for turn in range(4)]
        for j, (dz, dy, dc) in enumerate(INNER):
            i = g * GROUP + j
            back = pltpu.make_async_remote_copy(
                yx.at[i], ret.at[expert], es.at[g], er.at[g],
                device_id={"sp": homes[j // 2], "dp": back_to[(dz + dy) % 4][dc]},
                device_id_type=MESH,
            )
            if j == OWN_AT:
                own = pltpu.make_async_copy(yx.at[i], ret.at[expert], er.at[g])
                pl.when(g != OWN_GROUP)(back.start)
                pl.when(g == OWN_GROUP)(own.start)
            else:
                back.start()

    def early(g, carry):
        arrive(g)
        work(g)
        return carry

    def late(g, carry):
        give_back(g)
        return carry

    lax.fori_loop(0, 3, early, 0)
    lax.fori_loop(0, 1, late, 0)
    arrive(3)
    lax.fori_loop(1, 3, late, 0)

    def last(g, carry):
        work(g)
        give_back(g)
        return carry

    lax.fori_loop(3, 4, last, 0)

    for g in range(4):
        whole_batch(yx, ret, es.at[g], er.at[g], GROUP).wait_recv()
    for n in range(D // NC):
        at = slice(n * NC, (n + 1) * NC)
        r = ret[:, :, at].reshape(SLOTS, NC)
        dims = (((0,), (0,)), ((), ()))
        moe = lax.dot_general(chigh[...], r, dims, preferred_element_type=F32)
        moe = moe + lax.dot_general(clow[...], r, dims, preferred_element_type=F32)
        out_ref[:, at] = (mid[:, at].astype(F32) + moe).astype(BF16)

    all_blocks(ka, ka, kvs.at[0], kvr.at[0], 15).wait_send()
    all_blocks(va, va, kvs.at[1], kvr.at[1], 15).wait_send()
    all_blocks(obuf, obuf, os_, or_, 15).wait_send()
    for g in range(4):
        count = GROUP - (g == OWN_GROUP)
        whole_batch(xs, rx, ds.at[g], dr.at[g], count).wait_send()
        whole_batch(yx, ret, es.at[g], er.at[g], count).wait_send()
    for i in range(STEPS):
        for b in range(2):
            to, copy = query_copy(i, b)
            if i == 0:
                pl.when(to != sp)(copy.wait_send)
            else:
                copy.wait_send()


def on_device(
    residual, query_maps, key_maps, value_rows, lambdas, head_gain, out_weight, ffn_gain,
    routes, route_weights, expert_gate, expert_up, expert_down,
):
    vmem = pl.BlockSpec(memory_space=pltpu.VMEM)
    smem = pl.BlockSpec(memory_space=pltpu.SMEM)
    hbm = pl.BlockSpec(memory_space=pl.ANY)
    score = pltpu.VMEM((QB, SEQ), F32)
    rows = pltpu.VMEM((SEQ, VD), BF16)
    tokens = pltpu.VMEM((TOK, D), BF16)
    table = pltpu.VMEM((SLOTS, TOK), BF16)
    slots = pltpu.VMEM((EXPERTS, CAP, D), BF16)
    sem = pltpu.SemaphoreType.DMA
    out = pl.pallas_call(
        layer_kernel,
        out_shape=pltpu.VMEM((TOK, D), BF16),
        in_specs=[hbm] * 4 + [smem] + [vmem] * 4 + [hbm] * 4,
        out_specs=vmem,
        scratch_shapes=[tokens] * 4 + [rows, rows, rows, score, score, score, score,
                        pltpu.VMEM((STEPS, QB, SEQ), BF16), pltpu.VMEM((STEPS, QB, 1), F32), rows, tokens,
                        pltpu.VMEM((TOK, D), F32), tokens,
                        table, table, table,
                        pltpu.VMEM((D, D), BF16), pltpu.VMEM((D, FF), BF16),
                        pltpu.VMEM((D, FF), BF16), pltpu.VMEM((FF, D), BF16),
                        slots, slots, pltpu.VMEM((GROUP * CAP, FF), BF16), slots, slots]
        + [sem((2,)), sem((2,)), sem((16,)), sem((16,)), sem, sem((STEPS,))] + [sem((4,))] * 7
        + [pltpu.SemaphoreType.REGULAR],
        compiler_params=pltpu.CompilerParams(
            collective_id=0, has_side_effects=True, vmem_limit_bytes=60 * 2**20
        ),
        name="layer",
    )(
        query_maps[0], key_maps[0], value_rows[0], residual[0], lambdas,
        head_gain.reshape(HEADS, VD), ffn_gain.reshape(1, D), routes[0].T, route_weights[0].T,
        out_weight, expert_gate[0], expert_up[0], expert_down[0],
    )
    return out[None]


def solution(mesh):
    tokens = P("dp", "sp", None)
    experts = P(("sp", "dp"), None, None)
    placed = (tokens,) * 4 + (P(),) * 4 + (tokens,) * 2 + (experts,) * 3
    return jax.shard_map(
        on_device, mesh=mesh, in_specs=placed, out_specs=tokens, check_vma=False
    )
```
